32 devices in a mesh: sp: 16 (over z, y, x), tp: 2 (over core).
Axes of the slice: x: 2, y: 2, z: 4, core: 2. Of those that a mesh axis runs over, the one named last changes fastest.
Arguments:
- stream: bfloat16 [4096, 2048], P('sp', 'tp'), may hold values from -80 to 80
- norm_gain: float32 [2048], P('tp'), may hold values from 0.1 to 1.9
- cotangent: bfloat16 [4096, 2048], P('sp', 'tp'), may hold values from -6 to 6
- route_weights: float32 [4096, 2], P('sp'), may hold values from 0.1 to 1.5
- routes: int32 [4096, 2], P('sp'), may hold values from 0 to 15, all different within a row; in each aligned block of 256 rows (0 to 255, 256 to 511, ...) at most 64 rows name the same one
- conv_input: bfloat16 [4096, 1024], P('sp', 'tp'), may hold values from -6 to 6
- conv_bgate: bfloat16 [4096, 1024], P('sp', 'tp'), may hold values from -6 to 6
- conv_cgate: bfloat16 [4096, 1024], P('sp', 'tp'), may hold values from -6 to 6
- conv_taps: float32 [3, 1024], P(None, 'tp'), may hold values from -3 to 3
- out_proj: bfloat16 [2048, 1024], P(None, 'tp'), may hold values from -0.1875 to 0.1875
- gate_weight: bfloat16 [16, 2048, 1024], P('sp', None, 'tp'), may hold values from -0.125 to 0.125
- up_weight: bfloat16 [16, 2048, 1024], P('sp', None, 'tp'), may hold values from -0.125 to 0.125
- down_weight: bfloat16 [16, 1024, 2048], P('sp', 'tp'), may hold values from -0.1875 to 0.1875
Outputs:
- stream_grad: bfloat16 [4096, 2048], P('sp', 'tp')
- proj_grad: float32 [2048, 1024], P('sp', 'tp')
- input_grad: bfloat16 [4096, 1024], P('sp', 'tp')
- bgate_grad: bfloat16 [4096, 1024], P('sp', 'tp')
- cgate_grad: bfloat16 [4096, 1024], P('sp', 'tp')
- gate_grad: float32 [16, 2048, 1024], P('sp', None, 'tp')
- up_grad: float32 [16, 2048, 1024], P('sp', None, 'tp')
- down_grad: float32 [16, 1024, 2048], P('sp', 'tp')
The draws below stay inside these ranges and needn't reach their ends.
Inputs may be any that keep to these rules, and one draw needn't show every extreme that they name: `routes`: the 2 experts of a token differ. Among the tokens of one index of sp, no expert is named more than 64 times, a bound that some block reaches.
All inputs are finite; a program needn't handle non-finite values.
Results may differ from the reference program's by a relative error of at most 0.003.
The reference program's roundings to bfloat16 on the way count: a program that leaves them out, or rounds other values in their place, can miss the bound.
Values may be sent and summed in bfloat16 or wider, within the bound.
A program may use at most 128 MiB of HBM per device.

```python
import math
import jax
import jax.numpy as jnp
import numpy as np
from jax import lax

D = 2048
CW = 1024
EH = 1024
K = 2
TOK_DEV = 256
TOKENS = 4096
EXPERTS = 16
CAP = 64
N_SP = 16
N_TP = 2


def draw_stream(key, part):
    keys = jax.random.split(key, 3)
    row_scale = jnp.exp(jax.random.uniform(keys[0], (TOKENS, 1), jnp.float32, 0.0, 2.3))
    column_rise = 3.0 ** (jnp.arange(D, dtype=jnp.float32) / D)
    column_scale = column_rise[None, :] * jnp.exp(jax.random.uniform(keys[1], (1, D), jnp.float32, -0.5, 0.5))
    values = jax.random.normal(keys[2], (TOKENS, D), jnp.float32)
    return jnp.clip(values * row_scale * column_scale, -80.0, 80.0).astype(jnp.bfloat16)


def spiked(array, key, source, target, parts, factor):
    def block_of(axis_at):
        return (jnp.arange(array.shape[axis_at]) // (array.shape[axis_at] // parts)).reshape((-1,) + (1,) * (array.ndim - 1 - axis_at))

    one_side = jax.random.permutation(key, parts)[block_of(target)]
    other_side = (block_of(target) + parts // 2) % parts
    return jnp.where((block_of(source) == one_side) | (block_of(source) == other_side), factor * array, array)


def steps_of(key, extent, shards, smallest, top_value):
    gain, own = 1.0, jax.random.fold_in(key, 6)
    for dim, parts in shards:
        steps = jnp.exp(jax.random.uniform(jax.random.fold_in(own, dim), (parts,), jnp.float32, smallest / len(shards), top_value / len(shards)))
        gain = gain * jnp.repeat(steps, extent[dim] // parts).reshape([-1 if axis == dim else 1 for axis in range(len(extent))])
    return gain


def shared_out(rng, own, number, rows, count, top, limit, slope):
    ranking = jax.random.permutation(rng, count)
    packed, ordinary = portions_of(count, rows * top, limit, slope, True), portions_of(count, rows * top, limit, slope, False)
    places = jnp.arange(count)

    def named(lengths, turn):
        used = int((lengths > 0).sum())
        fixed = max(1, used // 4)
        shifted = fixed + (places - fixed + turn * (used - fixed)) % max(1, count - fixed)
        return jnp.zeros((count,), jnp.int32).at[ranking[jnp.where(places < fixed, places, shifted)]].set(jnp.asarray(lengths, jnp.int32))

    lengths = jnp.where(number % 4 == 0, named(packed, number // 4), named(ordinary, number - number // 4 - 1))
    mixed = jax.random.permutation(jax.random.fold_in(own, 3), count)
    source_of, sink = mixed[0:count // 2 * 2:2], mixed[1:count // 2 * 2:2]
    room = jnp.minimum(lengths[source_of] - 1, limit - lengths[sink]) // 2
    room = jnp.where((source_of == ranking[0]) | (sink == ranking[0]) | (lengths[sink] == 0), 0, jnp.maximum(room, 0))
    shifted = jax.random.randint(jax.random.fold_in(own, 4), (count // 2,), 0, 1 << 20) % (room + 1)
    lengths = lengths.at[source_of].add(-shifted).at[sink].add(shifted)
    members = jnp.searchsorted(jnp.cumsum(lengths), jnp.arange(rows * top), side="right").astype(jnp.int32)
    grid = members.reshape(top, rows).T
    grid = grid[jax.random.permutation(jax.random.fold_in(own, 1), rows)]
    turn = jax.random.randint(jax.random.fold_in(own, 2), (rows, 1), 0, top)
    return jnp.take_along_axis(grid, (jnp.arange(top)[None, :] + turn) % top, axis=1)


def portions_of(amount, total, bound, lean, full):
    loads = [(1 << 20) // math.isqrt(standing ** lean) + 1 for standing in range(1, amount + 1)]
    largest = bound if full else min(bound, max(-(-total // amount), total * loads[0] // sum(loads)))
    least = 1 if total - largest >= amount - 1 else 0
    given, spare = [largest] + [least] * (amount - 1), total - largest - least * (amount - 1)
    while spare > 0:
        candidates = [i for i in range(1, amount) if given[i] < largest] or [i for i in range(1, amount) if given[i] < bound]
        mass, left = sum([loads[i] for i in candidates]), spare
        for i in candidates:
            extra = min(bound - given[i], max(1, left * loads[i] // mass), spare)
            given[i] = given[i] + extra
            spare = spare - extra
    return np.array(given)


def gaussian(stream_key, extent, spread, limit, pieces=(), kind=jnp.bfloat16):
    loudness = steps_of(stream_key, extent, pieces, -0.22, 0.18) if pieces else 1.0
    result = jax.random.normal(stream_key, extent, jnp.float32) * spread * loudness
    return jnp.minimum(jnp.maximum(result, -limit), limit).astype(kind)


def noise_with(own_key, extent, scale, bound, pieces, heavy, kind=jnp.bfloat16):
    entries = scale * jax.random.normal(own_key, extent, jnp.float32)
    if pieces:
        entries = entries * steps_of(own_key, extent, pieces, -0.22, 0.18)
    return jnp.clip(spiked(entries, jax.random.fold_in(own_key, 3), *heavy), -bound, bound).astype(kind)


def setup_inputs(seed: int = 0) -> dict:
    splits = jax.random.split(jax.random.key(seed), 14)
    stream = draw_stream(jax.random.fold_in(splits[13], 71), 0)
    norm_gain = jnp.clip(1.0 + 0.18 * jax.random.normal(splits[1], (D,), jnp.float32), 0.1, 1.9)
    cotangent = noise_with(splits[2], (TOKENS, D), 1.0, 6.0, ((0, 16), (1, 2)), (0, 1, 16, 2.0))
    route_weights = jnp.clip(0.1 + 1.4 * jax.random.uniform(splits[3], (TOKENS, K), jnp.float32) ** steps_of(splits[3], (TOKENS, K), ((0, 16),), -0.2, 0.2), 0.1, 1.5)
    routes_keys = jax.random.split(jax.random.fold_in(splits[4], 1), TOKENS // TOK_DEV)
    routes_turns = jax.random.permutation(jax.random.fold_in(splits[4], 3), TOKENS // TOK_DEV)
    routes = jax.vmap(lambda own, number: shared_out(jax.random.fold_in(splits[4], 2), own, number, TOK_DEV, EXPERTS, K, CAP, 1))(routes_keys, routes_turns).reshape((TOKENS, K))
    conv_input = gaussian(splits[5], (TOKENS, CW), 1.0, 6.0, ((0, 16), (1, 2)))
    conv_bgate = gaussian(splits[6], (TOKENS, CW), 1.0, 6.0, ((0, 16), (1, 2)))
    conv_cgate = gaussian(splits[7], (TOKENS, CW), 1.0, 6.0, ((0, 16), (1, 2)))
    conv_taps = gaussian(splits[8], (3, CW), 0.5, 3.0, ((1, 2),), jnp.float32)
    out_proj = gaussian(splits[9], (D, CW), CW ** -0.5, 0.1875, ((1, 2),))
    gate_weight = gaussian(splits[10], (EXPERTS, D, EH), D ** -0.5, 0.125, ((0, 16), (2, 2)))
    up_weight = gaussian(splits[11], (EXPERTS, D, EH), D ** -0.5, 0.125, ((0, 16), (2, 2)))
    down_weight = gaussian(splits[12], (EXPERTS, EH, D), EH ** -0.5, 0.1875, ((0, 16), (1, 2)))
    return {"stream": stream, "norm_gain": norm_gain, "cotangent": cotangent, "route_weights": route_weights, "routes": routes, "conv_input": conv_input, "conv_bgate": conv_bgate, "conv_cgate": conv_cgate, "conv_taps": conv_taps, "out_proj": out_proj, "gate_weight": gate_weight, "up_weight": up_weight, "down_weight": down_weight}


EPSILON = 1e-06

def expert_backward(inputs, grads_out, gate_w, up_w, down_w):
    gate_lin = jnp.dot(inputs, gate_w, preferred_element_type=jnp.float32)
    up_lin = jnp.dot(inputs, up_w, preferred_element_type=jnp.float32)
    sigmoid_gate = jax.nn.sigmoid(gate_lin)
    silu_gate = gate_lin * sigmoid_gate
    hidden = (silu_gate * up_lin).astype(jnp.bfloat16)
    down_g = jnp.dot(hidden.T, grads_out, preferred_element_type=jnp.float32)
    hidden_grad = jnp.dot(grads_out, down_w.T, preferred_element_type=jnp.float32)
    gate_pre = (hidden_grad * up_lin * sigmoid_gate * (1.0 + gate_lin * (1.0 - sigmoid_gate))).astype(jnp.bfloat16)
    up_pre = (hidden_grad * silu_gate).astype(jnp.bfloat16)
    gate_g = jnp.dot(inputs.T, gate_pre, preferred_element_type=jnp.float32)
    up_g = jnp.dot(inputs.T, up_pre, preferred_element_type=jnp.float32)
    return (gate_g, up_g, down_g, gate_pre, up_pre)

def reference(stream, norm_gain, cotangent, route_weights, routes, conv_input, conv_bgate, conv_cgate, conv_taps, out_proj, gate_weight, up_weight, down_weight):
    stream_float = stream.astype(jnp.float32)
    inverse = lax.rsqrt(lax.optimization_barrier(jnp.mean(stream_float * stream_float, axis=1, keepdims=True)) + EPSILON)
    normed = (stream_float * inverse * norm_gain[None, :]).astype(jnp.bfloat16)
    cot_float = cotangent.astype(jnp.float32)
    weighted = (route_weights[:, :, None] * cot_float[:, None, :]).astype(jnp.bfloat16).reshape(TOKENS * K, D)
    blocks = routes.reshape(N_SP, TOK_DEV * K).astype(jnp.int32)
    onehot = (blocks[:, :, None] == jnp.arange(EXPERTS, dtype=jnp.int32)[None, None, :]).astype(jnp.int32)
    earlier = jnp.cumsum(onehot, axis=1) - onehot
    position = lax.optimization_barrier(jnp.sum(earlier * onehot, axis=2)).astype(jnp.int32)
    source = jnp.arange(N_SP, dtype=jnp.int32)[:, None]
    arrival = (source * CAP + position).astype(jnp.int32)
    assign_ids = jnp.arange(TOKENS * K, dtype=jnp.int32).reshape(N_SP, TOK_DEV * K)
    table = jnp.full((EXPERTS, N_SP * CAP), TOKENS * K, jnp.int32).at[blocks, arrival].set(assign_ids)
    normed_pad = jnp.concatenate([normed, jnp.zeros((1, D), jnp.bfloat16)], axis=0)
    weighted_pad = jnp.concatenate([weighted, jnp.zeros((1, D), jnp.bfloat16)], axis=0)
    half_width = EH // N_TP

    def one_expert(operands):
        slot_ids, gate_w, up_w, down_w = operands
        token_ids = (slot_ids // K).astype(jnp.int32)
        inputs = normed_pad[token_ids]
        grads_out = weighted_pad[slot_ids]
        gate_g, up_g, down_g, gate_pre, up_pre = expert_backward(inputs, grads_out, gate_w, up_w, down_w)
        summed = jnp.zeros((N_SP * CAP, D), jnp.float32)
        for part_index in range(N_TP):
            low_col = part_index * half_width
            partial_value = jnp.dot(gate_pre[:, low_col:low_col + half_width], gate_w[:, low_col:low_col + half_width].T, preferred_element_type=jnp.float32)
            partial_value = partial_value + jnp.dot(up_pre[:, low_col:low_col + half_width], up_w[:, low_col:low_col + half_width].T, preferred_element_type=jnp.float32)
            rounded = lax.optimization_barrier(partial_value.astype(jnp.bfloat16))
            summed = summed + rounded.astype(jnp.float32)
        return (gate_g, up_g, down_g, summed.astype(jnp.bfloat16))
    gate_grad, up_grad, down_grad, slot_grads = lax.map(one_expert, (table, gate_weight, up_weight, down_weight))
    token_index = (table.reshape(-1) // K).astype(jnp.int32)
    normed_grad = jnp.zeros((TOKENS + 1, D), jnp.float32).at[token_index].add(slot_grads.reshape(-1, D).astype(jnp.float32))[:TOKENS]
    cross = lax.optimization_barrier(jnp.sum(stream_float * norm_gain[None, :] * normed_grad, axis=1, keepdims=True))
    stream_grad = (cot_float + inverse * norm_gain[None, :] * normed_grad - stream_float * inverse * inverse * inverse * cross / D).astype(jnp.bfloat16)
    input_float = conv_input.astype(jnp.float32)
    cgate_float = conv_cgate.astype(jnp.float32)
    bgate_float = conv_bgate.astype(jnp.float32)
    gated = cgate_float * input_float
    padded = jnp.pad(gated, ((2, 0), (0, 0)))
    conv_out = conv_taps[0][None, :] * padded[:-2] + conv_taps[1][None, :] * padded[1:-1] + conv_taps[2][None, :] * padded[2:]
    mixer_out = (bgate_float * conv_out).astype(jnp.bfloat16)
    proj_grad = lax.dot_general(stream_grad, mixer_out, (((0,), (0,)), ((), ())), preferred_element_type=jnp.float32)
    mixer_grad = jnp.dot(stream_grad, out_proj, preferred_element_type=jnp.float32)
    delta = mixer_grad * bgate_float
    padded_back = jnp.pad(delta, ((0, 2), (0, 0)))
    gated_grad = conv_taps[2][None, :] * padded_back[:-2] + conv_taps[1][None, :] * padded_back[1:-1] + conv_taps[0][None, :] * padded_back[2:]
    bgate_grad = (mixer_grad * conv_out).astype(jnp.bfloat16)
    input_grad = (gated_grad * cgate_float).astype(jnp.bfloat16)
    cgate_grad = (gated_grad * input_float).astype(jnp.bfloat16)
    return (stream_grad, proj_grad, input_grad, bgate_grad, cgate_grad, gate_grad, up_grad, down_grad)
```

```python
import jax
import jax.numpy as jnp
from jax import lax
from jax.experimental import pallas as pl
from jax.experimental.pallas import tpu as pltpu
from jax.sharding import PartitionSpec as P

D = 2048


EPSILON = 1e-06


def shifted(value, axis, steps):
    count = lax.axis_size(axis)
    leading, last = (max(0, -steps), min(count, count - steps))
    return lax.ppermute(value, axis, [(source, source + steps) for source in range(leading, last)])


def contract_rows(left, right):
    return lax.dot_general(
        left, right, (((0,), (0,)), ((), ())), preferred_element_type=jnp.float32
    )


def contract_cols(left, right):
    return lax.dot_general(
        left, right, (((1,), (1,)), ((), ())), preferred_element_type=jnp.float32
    )


MESH = pl.DeviceIdType.MESH


def greet(count, peer_of, other=None):
    barrier = pltpu.get_barrier_semaphore()

    @pl.loop(1, count)
    def _(i):
        pl.semaphore_signal(barrier, inc=1, device_id={"sp": peer_of(i)}, device_id_type=MESH)

    if other is not None:
        pl.semaphore_signal(barrier, inc=1, device_id={"tp": other}, device_id_type=MESH)
    pl.semaphore_wait(barrier, count - 1 if other is None else count)


def expert_kernel(
    planes,
    group,
    stream_hbm,
    gain_ref,
    cot_hbm,
    route_ref,
    u_hbm,
    b_hbm,
    c_hbm,
    taps_ref,
    gate_hbm,
    up_hbm,
    down_hbm,
    ret_ref,
    gate_out,
    up_out,
    down_out,
    slot_ref,
    inv_ref,
    conv_ref,
    near_ref,
    column,
    outgoing,
    rows_ref,
    gate_w,
    up_w,
    down_w,
    hidden_ref,
    gate_pre_ref,
    up_pre_ref,
    part_ref,
    theirs_ref,
    sum_ref,
    stream_ref,
    u_ref,
    b_ref,
    c_ref,
    rim_ref,
    mixed_ref,
    small_ref,
    square_ref,
    square_other,
    select_ref,
    scale_ref,
    load,
    hop_send,
    hop_recv,
    plane_send,
    plane_recv,
    cross_send,
    cross_recv,
    part_send,
    part_recv,
    back_send,
    back_recv,
    small_send,
    small_recv,
    rim_send,
    rim_recv,
    square_send,
    square_recv,
    mixed_send,
    mixed_recv,
):
    count = planes * group
    me = lax.axis_index("sp")
    side = lax.axis_index("tp")
    other = 1 - side
    here = lax.div(me, group)
    place = lax.rem(me, group)
    tokens = stream_ref.shape[0]
    width = column.shape[3]
    bunch = outgoing.shape[2]
    capacity = bunch // group
    f32, bf16 = jnp.float32, jnp.bfloat16

    def local(i, source, target):
        return pltpu.make_async_copy(source, target, load.at[i])

    def remote(source, target, sent, received, **peer):
        return pltpu.make_async_remote_copy(
            src_ref=source,
            dst_ref=target,
            send_sem=sent,
            recv_sem=received,
            device_id=peer,
            device_id_type=MESH,
        )

    loads = [
        local(0, cot_hbm.at[:, 0:width], column.at[here, 0]),
        local(1, cot_hbm.at[:, width : 2 * width], column.at[here, 1]),
        local(2, stream_hbm, stream_ref),
        local(3, u_hbm, u_ref),
        local(4, c_hbm, c_ref),
        local(5, b_hbm, b_ref),
        local(6, gate_hbm, gate_w),
        local(7, up_hbm, up_w),
        local(8, down_hbm, down_w),
    ]
    for copy in loads:
        copy.start()

    def hop(way, block, piece):
        spot = column.at[block, piece]
        return remote(
            spot,
            spot,
            hop_send.at[way, block, piece],
            hop_recv.at[block, piece],
            sp=me + (1 - 2 * way) * group,
        )

    def onward(way, block, piece):
        room = here < planes - 1 if way == 0 else here > 0

        @pl.when(room)
        def _():
            hop(way, block, piece).start()

    def small(i):
        return remote(
            small_ref.at[here],
            small_ref.at[here],
            small_send.at[i],
            small_recv.at[i],
            sp=lax.rem(here + i, planes) * group + place,
        )

    def small_from(i):
        return remote(
            small_ref.at[here],
            small_ref.at[lax.rem(here + planes - i, planes)],
            small_send.at[i],
            small_recv.at[i],
            sp=lax.rem(here + i, planes) * group + place,
        )

    def stripe(piece):
        return lax.div(piece, 2), 2 * side + lax.rem(piece, 2)

    def span(start, size):
        return pl.ds(pl.multiple_of(start, size), size)

    def inplane(block, piece, i):
        target = lax.rem(place + i, group)
        kind, part = stripe(piece)
        return remote(
            outgoing.at[block, piece, span(target * capacity, capacity)],
            rows_ref.at[kind, part, span(block * bunch + place * capacity, capacity)],
            plane_send.at[block, piece, i],
            plane_recv.at[block, piece, i],
            sp=here * group + target,
        )

    def cross(block, piece):
        kind, part = stripe(piece)
        spot = rows_ref.at[kind, part, span(block * bunch, bunch)]
        return remote(
            spot, spot, cross_send.at[block, piece], cross_recv.at[block, piece], tp=other
        )

    def part_copy(block, half):
        return remote(
            part_ref.at[block, :, half * width : (half + 1) * width],
            theirs_ref.at[block, :, half * width : (half + 1) * width],
            part_send.at[block, half],
            part_recv.at[block, half],
            tp=other,
        )

    def back(block, i):
        return remote(
            sum_ref.at[block, span(i * capacity, capacity)],
            ret_ref.at[span(me * capacity, capacity)],
            back_send.at[block, i],
            back_recv.at[me],
            sp=block * group + i,
        )

    def back_from(source):
        return remote(
            sum_ref.at[0, pl.ds(0, capacity)],
            ret_ref.at[span(source * capacity, capacity)],
            back_send.at[0, 0],
            back_recv.at[source],
            sp=source,
        )

    rim = rim_ref.shape[1]

    def rim_copy(i):
        source = (u_ref, c_ref)[i]
        return remote(
            source.at[tokens - rim : tokens],
            rim_ref.at[i],
            rim_send.at[i],
            rim_recv.at[i],
            sp=me + 1,
        )

    def mixed(i):
        return remote(
            mixed_ref,
            near_ref.at[span(place * tokens, tokens)],
            mixed_send.at[i],
            mixed_recv.at[i],
            sp=here * group + lax.rem(place + i, group),
        )

    square_copy = remote(square_ref, square_other, square_send, square_recv, tp=other)

    def prepare(block, way):
        wanted = lax.broadcasted_iota(jnp.int32, (bunch, tokens), 0) + here * bunch
        wanted = wanted.astype(f32)
        first = wanted == small_ref[block, 0:1, :]
        second = wanted == small_ref[block, 1:2, :]
        select_ref[way] = jnp.where(first | second, 1.0, 0.0).astype(bf16)
        weight = jnp.where(first, small_ref[block, 2:3, :], 0.0) + jnp.where(
            second, small_ref[block, 3:4, :], 0.0
        )
        scale = jnp.sum(weight, axis=1, keepdims=True)
        scale_ref[way] = jnp.broadcast_to(scale, (bunch, scale_ref.shape[2]))

    def pick(block, way, piece):
        chosen = jnp.dot(select_ref[way], column[block, piece], preferred_element_type=f32)
        scale = jnp.where(piece < 2, scale_ref[way][:, 0:1], 1.0)
        outgoing[block, piece] = (chosen * scale).astype(bf16)
        kind, part = stripe(piece)
        rows_ref[kind, part, span(block * bunch + place * capacity, capacity)] = outgoing[
            block, piece, span(place * capacity, capacity)
        ]

        @pl.loop(1, group)
        def _(i):
            inplane(block, piece, i).start()

    greet(count, lambda i: lax.rem(me + i, count), other)
    for piece in range(2):
        loads[piece].wait()
        for way in range(2):
            onward(way, here, piece)
    loads[2].wait()
    stream = stream_ref[...].astype(f32)
    lanes = square_ref.shape[1]
    total = jnp.zeros((tokens, lanes), f32)
    for start in range(0, 2 * width, lanes):
        piece_value = stream[:, start : start + lanes]
        total = total + piece_value * piece_value
    square_ref[...] = total
    square_copy.start()
    for i in range(3, 5):
        loads[i].wait()

    @pl.when(me < count - 1)
    def _():
        for i in range(2):
            rim_copy(i).start()

    @pl.when(me == 0)
    def _():
        rim_ref[...] = jnp.zeros_like(rim_ref)

    expert_row = lax.broadcasted_iota(jnp.int32, (count, tokens), 0).astype(f32)
    named = [jnp.where(expert_row == route_ref[k : k + 1, :], 1.0, 0.0) for k in range(2)]
    earlier = lax.broadcasted_iota(jnp.int32, (tokens, tokens), 0) < lax.broadcasted_iota(
        jnp.int32, (tokens, tokens), 1
    )
    before = jnp.dot(
        (named[0] + named[1]).astype(bf16),
        jnp.where(earlier, 1.0, 0.0).astype(bf16),
        preferred_element_type=f32,
    )
    slots = [
        route_ref[k : k + 1, :] * capacity + jnp.sum(named[k] * before, axis=0, keepdims=True)
        for k in range(2)
    ]
    info = jnp.concatenate(slots + [route_ref[2:8, :]], axis=0)
    small_ref[here] = info
    slot_ref[...] = info

    @pl.loop(1, planes)
    def _(i):
        small(i).start()

    prepare(here, 0)
    for piece in range(2):
        pick(here, 0, piece)
    square_copy.wait_recv()
    total = square_ref[...] + square_other[...]
    inverse = lax.rsqrt(jnp.sum(total, axis=1, keepdims=True) / (4 * width) + EPSILON)
    inv_ref[...] = jnp.broadcast_to(inverse, inv_ref.shape)
    for piece in range(2):
        cols = slice(piece * width, (piece + 1) * width)
        value = stream_ref[:, cols].astype(f32) * inverse * gain_ref[:, cols]
        column[here, 2 + piece] = value.astype(bf16)
    for piece in range(2, 4):
        for way in range(2):
            onward(way, here, piece)
    for piece in range(2, 4):
        pick(here, 0, piece)

    @pl.when(me > 0)
    def _():
        for i in range(2):
            rim_copy(i).wait_recv()

    loads[5].wait()
    gated = c_ref[...].astype(f32) * u_ref[...].astype(f32)
    rim_gated = rim_ref[1].astype(f32) * rim_ref[0].astype(f32)
    row = lax.broadcasted_iota(jnp.int32, gated.shape, 0)
    one = jnp.where(row == 0, rim_gated[rim - 1 : rim], pltpu.roll(gated, 1, 0))
    two = jnp.where(
        row == 0,
        rim_gated[rim - 2 : rim - 1],
        jnp.where(row == 1, rim_gated[rim - 1 : rim], pltpu.roll(gated, 2, 0)),
    )
    conv = taps_ref[0:1, :] * two + taps_ref[1:2, :] * one + taps_ref[2:3, :] * gated
    conv_ref[...] = conv
    mixed_value = (b_ref[...].astype(f32) * conv).astype(bf16)
    mixed_ref[...] = mixed_value
    near_ref[span(place * tokens, tokens)] = mixed_value

    @pl.loop(1, group)
    def _(i):
        mixed(i).start()

    @pl.loop(1, planes)
    def _(i):
        small_from(i).wait_recv()

    for i in range(6, 9):
        loads[i].wait()

    def arrive(step, piece):
        for way in range(2):
            block = here - step if way == 0 else here + step
            valid = (step < planes) & (block >= 0) & (block < planes)

            @pl.when(valid)
            def _():
                hop(way, block, piece).wait_recv()
                onward(way, block, piece)

        for way in range(2):
            block = here - step if way == 0 else here + step
            valid = (step < planes) & (block >= 0) & (block < planes)

            @pl.when(valid)
            def _():
                @pl.when(piece == 0)
                def _():
                    prepare(block, way)

                pick(block, way, piece)

    def gather(step, way):
        block = here - step + 2 * way * step
        valid = (block >= 0) & (block < planes) & ((way == 0) | (step > 0))

        @pl.when(valid)
        def _():
            @pl.loop(0, 4)
            def _(piece):
                @pl.loop(1, group)
                def _(i):
                    inplane(block, piece, i).wait_recv()

                cross(block, piece).start()

    def compute(step, way):
        block = here - step + 2 * way * step
        valid = (block >= 0) & (block < planes) & ((way == 0) | (step > 0))

        @pl.when(valid)
        def _():
            @pl.loop(0, 4)
            def _(piece):
                cross(block, piece).wait_recv()

            rows = span(block * bunch, bunch)
            gate_lin = jnp.zeros((bunch, gate_w.shape[1]), f32)
            up_lin = jnp.zeros((bunch, gate_w.shape[1]), f32)
            hidden_grad = jnp.zeros((bunch, gate_w.shape[1]), f32)
            for part in range(4):
                cols = slice(part * width, (part + 1) * width)
                inputs = rows_ref[1, part, rows]
                gate_lin += jnp.dot(inputs, gate_w[cols], preferred_element_type=f32)
                up_lin += jnp.dot(inputs, up_w[cols], preferred_element_type=f32)
                hidden_grad += contract_cols(rows_ref[0, part, rows], down_w[:, cols])
            sigmoid_gate = jax.nn.sigmoid(gate_lin)
            silu_gate = gate_lin * sigmoid_gate
            hidden_ref[rows] = (silu_gate * up_lin).astype(bf16)
            gate_pre = (
                hidden_grad * up_lin * sigmoid_gate * (1.0 + gate_lin * (1.0 - sigmoid_gate))
            ).astype(bf16)
            up_pre = (hidden_grad * silu_gate).astype(bf16)
            gate_pre_ref[rows] = gate_pre
            up_pre_ref[rows] = up_pre

            def partial(whose, half):
                spot = span((2 * whose + half) * width, width)
                value = contract_cols(gate_pre_ref[rows], gate_w[spot])
                value += contract_cols(up_pre_ref[rows], up_w[spot])
                return value.astype(bf16)

            for half in range(2):
                part_ref[block, :, half * width : (half + 1) * width] = partial(other, half)
                part_copy(block, half).start()
            for half in range(2):
                cols = slice(half * width, (half + 1) * width)
                mine = partial(side, half).astype(f32)
                part_copy(block, half).wait_recv()
                theirs = theirs_ref[block, :, cols].astype(f32)
                sum_ref[block, :, cols] = (mine + theirs).astype(bf16)

            @pl.loop(0, group)
            def _(i):
                @pl.when(block * group + i != me)
                def _():
                    back(block, i).start()

                @pl.when(block * group + i == me)
                def _():
                    ret_ref[span(me * capacity, capacity)] = sum_ref[
                        block, span(i * capacity, capacity)
                    ]

    @pl.loop(1, planes + 1)
    def _(step):
        arrive(step, 0)

        @pl.loop(0, 2)
        def _(way):
            gather(step - 1, way)

        @pl.loop(0, 2)
        def _(way):
            compute(step - 1, way)

        @pl.loop(1, 4)
        def _(piece):
            arrive(step, piece)

    @pl.loop(0, 4)
    def _(part):
        inputs = rows_ref[1, part]
        spot = span(part * width, width)
        gate_out[spot] = contract_rows(inputs, gate_pre_ref[...])
        up_out[spot] = contract_rows(inputs, up_pre_ref[...])
        down_out[:, spot] = contract_rows(hidden_ref[...], rows_ref[0, part])

    @pl.loop(0, count)
    def _(source):
        @pl.when(source != me)
        def _():
            back_from(source).wait_recv()

    @pl.loop(0, planes)
    def _(block):
        @pl.loop(0, 4)
        def _(piece):
            for way in range(2):
                room = here < planes - 1 if way == 0 else here > 0
                mine = block <= here if way == 0 else block >= here

                @pl.when(room & mine)
                def _():
                    hop(way, block, piece).wait_send()

            cross(block, piece).wait_send()

            @pl.loop(1, group)
            def _(i):
                inplane(block, piece, i).wait_send()

        for half in range(2):
            part_copy(block, half).wait_send()

        @pl.loop(0, group)
        def _(i):
            @pl.when(block * group + i != me)
            def _():
                back(block, i).wait_send()

    @pl.loop(1, planes)
    def _(i):
        small(i).wait_send()

    @pl.loop(1, group)
    def _(i):
        mixed(i).wait()

    @pl.when(me < count - 1)
    def _():
        for i in range(2):
            rim_copy(i).wait_send()

    square_copy.wait_send()


def experts_pass(
    group, stream, gain, cotangent, route, u, b, c, taps, gate_w, up_w, down_w
):
    count = lax.axis_size("sp")
    planes = count // group
    tokens, features = stream.shape
    width = features // 2
    channels = u.shape[1]
    hidden = gate_w.shape[1]
    capacity = 4 * tokens // count
    bunch = group * capacity
    f32, bf16 = jnp.float32, jnp.bfloat16
    shape = jax.ShapeDtypeStruct
    outs = (
        shape((count * capacity, features), bf16),
        shape(gate_w.shape, f32),
        shape(up_w.shape, f32),
        shape(down_w.shape, f32),
        shape((8, tokens), f32),
        shape((tokens, 128), f32),
        shape((tokens, channels), f32),
        shape((group * tokens, channels), bf16),
    )
    vmem, anywhere = pl.BlockSpec(memory_space=pltpu.VMEM), pl.BlockSpec(memory_space=pl.ANY)
    dma = pltpu.SemaphoreType.DMA
    return pl.pallas_call(
        lambda *refs: expert_kernel(planes, group, *refs),
        out_shape=outs,
        in_specs=[
            anywhere,
            vmem,
            anywhere,
            vmem,
            anywhere,
            anywhere,
            anywhere,
            vmem,
            anywhere,
            anywhere,
            anywhere,
        ],
        out_specs=[vmem] * 8,
        scratch_shapes=[
            pltpu.VMEM((planes, 4, tokens, width), bf16),
            pltpu.VMEM((planes, 4, bunch, width), bf16),
            pltpu.VMEM((2, 4, planes * bunch, width), bf16),
            pltpu.VMEM(gate_w.shape, bf16),
            pltpu.VMEM(up_w.shape, bf16),
            pltpu.VMEM(down_w.shape, bf16),
            pltpu.VMEM((planes * bunch, hidden), bf16),
            pltpu.VMEM((planes * bunch, hidden), bf16),
            pltpu.VMEM((planes * bunch, hidden), bf16),
            pltpu.VMEM((planes, bunch, features), bf16),
            pltpu.VMEM((planes, bunch, features), bf16),
            pltpu.VMEM((planes, bunch, features), bf16),
            pltpu.VMEM((tokens, features), bf16),
            pltpu.VMEM((tokens, channels), bf16),
            pltpu.VMEM((tokens, channels), bf16),
            pltpu.VMEM((tokens, channels), bf16),
            pltpu.VMEM((2, 16, channels), bf16),
            pltpu.VMEM((tokens, channels), bf16),
            pltpu.VMEM((planes, 8, tokens), f32),
            pltpu.VMEM((tokens, 128), f32),
            pltpu.VMEM((tokens, 128), f32),
            pltpu.VMEM((2, bunch, tokens), bf16),
            pltpu.VMEM((2, bunch, 128), f32),
            dma((9,)),
            dma((2, planes, 4)),
            dma((planes, 4)),
            dma((planes, 4, group)),
            dma((planes, 4, group)),
            dma((planes, 4)),
            dma((planes, 4)),
            dma((planes, 2)),
            dma((planes, 2)),
            dma((planes, group)),
            dma((count,)),
            dma((planes,)),
            dma((planes,)),
            dma((2,)),
            dma((2,)),
            dma,
            dma,
            dma((group,)),
            dma((group,)),
        ],
        compiler_params=pltpu.CompilerParams(
            collective_id=0, has_side_effects=True, vmem_limit_bytes=60 * 2**20
        ),
        name="experts",
    )(stream, gain, cotangent, route, u, b, c, taps, gate_w, up_w, down_w)


def spread_kernel(count, step, x_ref, o_ref, send, recv, own):
    me = lax.axis_index("sp")
    side = lax.axis_index("tp")
    here = lax.rem(lax.div(me, step), count)
    block = x_ref.shape[0] // count

    def rows(index):
        return pl.ds(pl.multiple_of(index * block, block), block)

    def slot(i):
        return lax.rem(here + i + side * (count - 2 * i), count)

    def peer_of(i):
        return me + (slot(i) - here) * step

    def remote(i):
        return pltpu.make_async_remote_copy(
            src_ref=x_ref.at[rows(slot(i))],
            dst_ref=o_ref.at[rows(here)],
            send_sem=send.at[i],
            recv_sem=recv.at[i],
            device_id={"sp": peer_of(i)},
            device_id_type=MESH,
        )

    greet(count, peer_of)

    @pl.loop(1, count)
    def _(i):
        remote(i).start()

    home = pltpu.make_async_copy(x_ref.at[rows(here)], o_ref.at[rows(here)], own)
    home.start()
    home.wait()

    @pl.loop(1, count)
    def _(i):
        remote(i).wait()


def spread(x, number, count, step):
    return pl.pallas_call(
        lambda *refs: spread_kernel(count, step, *refs),
        out_shape=jax.ShapeDtypeStruct(x.shape, x.dtype),
        in_specs=[pl.BlockSpec(memory_space=pltpu.VMEM)],
        out_specs=pl.BlockSpec(memory_space=pltpu.VMEM),
        scratch_shapes=[pltpu.SemaphoreType.DMA((count,))] * 2 + [pltpu.SemaphoreType.DMA],
        compiler_params=pltpu.CompilerParams(
            collective_id=number, has_side_effects=True, vmem_limit_bytes=24 * 2**20
        ),
        name="spread%d" % number,
    )(x)


def local(
    stream,
    norm_gain,
    cotangent,
    route_weights,
    routes,
    conv_input,
    conv_bgate,
    conv_cgate,
    conv_taps,
    out_proj,
    gate_weight,
    up_weight,
    down_weight,
):
    experts = lax.axis_size("sp")
    tok_count = stream.shape[0]
    group = 2 ** ((experts.bit_length() - 1) // 2)
    stages = experts // group
    route = jnp.concatenate(
        [
            routes.astype(jnp.float32).T,
            route_weights.T,
            jnp.zeros((4, tok_count), jnp.float32),
        ],
        axis=0,
    )
    returned, gate_g, up_g, down_g, slots, inverse, conv_out, mixer_near = experts_pass(
        group,
        stream,
        norm_gain[None, :],
        cotangent,
        route,
        conv_input,
        conv_bgate,
        conv_cgate,
        conv_taps,
        gate_weight[0],
        up_weight[0],
        down_weight[0],
    )
    side = lax.axis_index("tp")
    stream_float = stream.astype(jnp.float32)
    cot_float = cotangent.astype(jnp.float32)
    gain_row = norm_gain[None, :]
    inverse = inverse[:, 0:1]
    input_float = conv_input.astype(jnp.float32)
    cgate_float = conv_cgate.astype(jnp.float32)
    bgate_float = conv_bgate.astype(jnp.float32)
    places = jnp.arange(returned.shape[0], dtype=jnp.int32).astype(jnp.float32)[:, None]
    token_select = ((places == slots[0:1]) | (places == slots[1:2])).astype(jnp.bfloat16)
    normed_grad = contract_rows(token_select, returned)
    cross = lax.psum(jnp.sum(stream_float * gain_row * normed_grad, axis=1), "tp")
    stream_grad = (
        cot_float
        + inverse * gain_row * normed_grad
        - stream_float * inverse * inverse * inverse * cross[:, None] / D
    ).astype(jnp.bfloat16)
    grad_other = lax.ppermute(stream_grad, "tp", [(0, 1), (1, 0)])
    grad_whole = jnp.concatenate(
        [
            jnp.where(side == 0, stream_grad, grad_other),
            jnp.where(side == 0, grad_other, stream_grad),
        ],
        axis=1,
    )
    columns = grad_whole.reshape(tok_count, stages, group, -1).transpose(2, 0, 1, 3)
    grad_near = spread(columns.reshape(group * tok_count, -1), 2, group, 1)
    shares = contract_rows(grad_near, mixer_near).astype(jnp.bfloat16)
    shares = spread(shares, 3, stages, group)
    shares = shares.reshape(stages, shares.shape[0] // stages, -1)
    proj_grad = jnp.sum(shares.astype(jnp.float32), axis=0)
    mixer_grad = jnp.dot(grad_whole, out_proj, preferred_element_type=jnp.float32)
    delta = mixer_grad * bgate_float
    next_rim = shifted(delta[:2], "sp", -1)
    extended_back = jnp.concatenate([delta, next_rim], axis=0)
    gated_grad = (
        conv_taps[2][None, :] * extended_back[:-2]
        + conv_taps[1][None, :] * extended_back[1:-1]
        + conv_taps[0][None, :] * extended_back[2:]
    )
    bgate_grad = (mixer_grad * conv_out).astype(jnp.bfloat16)
    input_grad = (gated_grad * cgate_float).astype(jnp.bfloat16)
    cgate_grad = (gated_grad * input_float).astype(jnp.bfloat16)
    return (
        stream_grad,
        proj_grad,
        input_grad,
        bgate_grad,
        cgate_grad,
        gate_g[None],
        up_g[None],
        down_g[None],
    )


def solution(mesh):
    return jax.shard_map(
        local,
        mesh=mesh,
        in_specs=(
            P("sp", "tp"),
            P("tp"),
            P("sp", "tp"),
            P("sp", None),
            P("sp", None),
            P("sp", "tp"),
            P("sp", "tp"),
            P("sp", "tp"),
            P(None, "tp"),
            P(None, "tp"),
            P("sp", None, "tp"),
            P("sp", None, "tp"),
            P("sp", "tp", None),
        ),
        out_specs=(
            P("sp", "tp"),
            P("sp", "tp"),
            P("sp", "tp"),
            P("sp", "tp"),
            P("sp", "tp"),
            P("sp", None, "tp"),
            P("sp", None, "tp"),
            P("sp", "tp", None),
        ),
        check_vma=False,
    )
```

```python
import jax
import jax.numpy as jnp
from jax import lax
from jax.experimental import pallas as pl
from jax.experimental.pallas import tpu as pltpu
from jax.sharding import PartitionSpec as P

EPSILON = 1e-06


def contract_rows(left, right):
    return lax.dot_general(
        left, right, (((0,), (0,)), ((), ())), preferred_element_type=jnp.float32
    )


def contract_cols(left, right):
    return lax.dot_general(
        left, right, (((1,), (1,)), ((), ())), preferred_element_type=jnp.float32
    )


MESH = pl.DeviceIdType.MESH
VMEM_LIMIT = 61 * 2**20


def layer_kernel(
    planes,
    group,
    stream_hbm,
    gain_ref,
    cot_hbm,
    weight_ref,
    route_ref,
    u_hbm,
    b_hbm,
    c_hbm,
    taps_ref,
    proj_hbm,
    gate_hbm,
    up_hbm,
    down_hbm,
    grad_hbm,
    proj_hbm_out,
    u_hbm_out,
    b_hbm_out,
    c_hbm_out,
    gate_out,
    up_out,
    down_out,
    column,
    outgoing,
    rows_ref,
    gate_w,
    up_w,
    down_w,
    hidden_ref,
    gate_pre_ref,
    up_pre_ref,
    part_ref,
    theirs_ref,
    ret_ref,
    stream_ref,
    u_ref,
    b_ref,
    c_ref,
    conv_ref,
    near_ref,
    rim_ref,
    mixed_ref,
    small_ref,
    square_ref,
    square_other,
    inner_ref,
    inner_other,
    select_ref,
    scale_ref,
    pull_ref,
    total_ref,
    grad_other,
    block_ref,
    share_ref,
    stack_ref,
    edge_ref,
    edge_next,
    grad_ref,
    proj_out,
    u_out,
    b_out,
    c_out,
    turn_ref,
    stage_ref,
    tall_ref,
    load,
    store,
    finish,
    hop_send,
    hop_recv,
    plane_send,
    plane_recv,
    cross_send,
    cross_recv,
    part_send,
    part_recv,
    back_send,
    back_recv,
    small_send,
    small_recv,
    rim_send,
    rim_recv,
    side_send,
    side_recv,
    mixed_send,
    mixed_recv,
    spread_send,
    spread_recv,
    pass_send,
    pass_recv,
    share_send,
    share_recv,
    edge_send,
    edge_recv,
):
    count = planes * group
    me = lax.axis_index("sp")
    side = lax.axis_index("tp")
    other = 1 - side
    here = lax.div(me, group)
    place = lax.rem(me, group)
    tokens = stream_ref.shape[0]
    width = column.shape[3]
    bunch = outgoing.shape[2]
    capacity = bunch // group
    f32, bf16 = jnp.float32, jnp.bfloat16

    def local(i, source, target):
        return pltpu.make_async_copy(source, target, load.at[i])

    def remote(source, target, sent, received, **peer):
        return pltpu.make_async_remote_copy(
            src_ref=source,
            dst_ref=target,
            send_sem=sent,
            recv_sem=received,
            device_id=peer,
            device_id_type=MESH,
        )

    loads = [
        local(0, cot_hbm.at[:, 0:width], column.at[here, 0]),
        local(1, cot_hbm.at[:, width : 2 * width], column.at[here, 1]),
        local(2, stream_hbm, stream_ref),
        local(3, u_hbm, u_ref),
        local(4, c_hbm, c_ref),
        local(5, b_hbm, b_ref),
        local(6, gate_hbm, gate_w),
        local(7, up_hbm, up_w),
        local(8, down_hbm, down_w),
        local(9, proj_hbm, gate_w),
    ]
    for copy in loads[:9]:
        copy.start()

    def hop(way, block, piece):
        spot = column.at[block, piece]
        return remote(
            spot,
            spot,
            hop_send.at[way, block, piece],
            hop_recv.at[block, piece],
            sp=me + (1 - 2 * way) * group,
        )

    def onward(way, block, piece):
        room = here < planes - 1 if way == 0 else here > 0

        @pl.when(room)
        def _():
            hop(way, block, piece).start()

    def small(i):
        return remote(
            small_ref.at[here],
            small_ref.at[here],
            small_send.at[i],
            small_recv.at[i],
            sp=lax.rem(here + i, planes) * group + place,
        )

    def small_from(i):
        return remote(
            small_ref.at[here],
            small_ref.at[lax.rem(here + planes - i, planes)],
            small_send.at[i],
            small_recv.at[i],
            sp=lax.rem(here + i, planes) * group + place,
        )

    def stripe(piece):
        return lax.div(piece, 2), 2 * side + lax.rem(piece, 2)

    def span(start, size):
        return pl.ds(pl.multiple_of(start, size), size)

    def inplane(block, piece, i):
        target = lax.rem(place + i, group)
        kind, part = stripe(piece)
        return remote(
            outgoing.at[block, piece, span(target * capacity, capacity)],
            rows_ref.at[kind, part, span(block * bunch + place * capacity, capacity)],
            plane_send.at[block, piece, i],
            plane_recv.at[block, piece, i],
            sp=here * group + target,
        )

    def cross(block, piece):
        kind, part = stripe(piece)
        spot = rows_ref.at[kind, part, span(block * bunch, bunch)]
        return remote(
            spot, spot, cross_send.at[block, piece], cross_recv.at[block, piece], tp=other
        )

    def part_copy(block, half):
        return remote(
            part_ref.at[block, :, half * width : (half + 1) * width],
            theirs_ref.at[block, :, half * width : (half + 1) * width],
            part_send.at[block, half],
            part_recv.at[block, half],
            tp=other,
        )

    def back(block, i):
        return remote(
            theirs_ref.at[block, span(i * capacity, capacity)],
            ret_ref.at[span(me * capacity, capacity)],
            back_send.at[block, i],
            back_recv.at[me],
            sp=block * group + i,
        )

    def back_from(source):
        return remote(
            theirs_ref.at[0, pl.ds(0, capacity)],
            ret_ref.at[span(source * capacity, capacity)],
            back_send.at[0, 0],
            back_recv.at[source],
            sp=source,
        )

    rim = rim_ref.shape[1]

    def rim_copy(i):
        source = (u_ref, c_ref)[i]
        return remote(
            source.at[tokens - rim : tokens],
            rim_ref.at[i],
            rim_send.at[i],
            rim_recv.at[i],
            sp=me + 1,
        )

    def mixed(i):
        return remote(
            mixed_ref,
            near_ref.at[span(place * tokens, tokens)],
            mixed_send.at[i],
            mixed_recv.at[i],
            sp=here * group + lax.rem(place + i, group),
        )

    def swap(i):
        mine, yours = (
            (square_ref, square_other),
            (inner_ref, inner_other),
            (grad_ref, grad_other),
        )[i]
        return remote(mine, yours, side_send.at[i], side_recv.at[i], tp=other)

    parts, sliver = block_ref.shape[0], block_ref.shape[2]
    per_part = planes // parts
    near = parts // 2
    depth = proj_out.shape[0]
    plain = per_part == 1

    def owned(part):
        return lax.div(part, near) == side

    def strip(target, part):
        if plain:
            start = ((part - side * near) * group + target) * sliver
        else:
            start = (target * near + part - side * near) * sliver
        return (grad_ref if plain else turn_ref).at[:, span(start, sliver)]

    def spread(target, part):
        return remote(
            strip(target, part),
            block_ref.at[part, span(place * tokens, tokens)],
            spread_send.at[target, part],
            spread_recv.at[place, part],
            sp=here * group + target,
        )

    def spread_from(source, part):
        return remote(
            grad_ref.at[:, pl.ds(0, sliver)],
            block_ref.at[part, span(source * tokens, tokens)],
            spread_send.at[source, part],
            spread_recv.at[source, part],
            sp=here * group + source,
        )

    def hand(part):
        spot = block_ref.at[part]
        return remote(spot, spot, pass_send.at[part], pass_recv.at[part], tp=other)

    def share(part, j):
        target = part * per_part + j
        return remote(
            share_ref.at[part, span(j * depth, depth)],
            stack_ref.at[here],
            share_send.at[part, j],
            share_recv.at[here],
            sp=target * group + place,
        )

    def share_from(source):
        return remote(
            share_ref.at[0, pl.ds(0, depth)],
            stack_ref.at[source],
            share_send.at[0, 0],
            share_recv.at[source],
            sp=source * group + place,
        )

    edge_copy = remote(edge_ref, edge_next, edge_send, edge_recv, sp=me - 1)


    def prepare(block, way):
        wanted = lax.broadcasted_iota(jnp.int32, (bunch, tokens), 0) + here * bunch
        wanted = wanted.astype(f32)
        first = wanted == small_ref[block, 0:1, :]
        second = wanted == small_ref[block, 1:2, :]
        select_ref[way] = jnp.where(first | second, 1.0, 0.0).astype(bf16)
        weight = jnp.where(first, small_ref[block, 2:3, :], 0.0) + jnp.where(
            second, small_ref[block, 3:4, :], 0.0
        )
        scale = jnp.sum(weight, axis=1, keepdims=True)
        scale_ref[way] = jnp.broadcast_to(scale, (bunch, scale_ref.shape[2]))

    def pick(block, way, piece):
        chosen = jnp.dot(select_ref[way], column[block, piece], preferred_element_type=f32)
        scale = jnp.where(piece < 2, scale_ref[way][:, 0:1], 1.0)
        outgoing[block, piece] = (chosen * scale).astype(bf16)
        kind, part = stripe(piece)
        rows_ref[kind, part, span(block * bunch + place * capacity, capacity)] = outgoing[
            block, piece, span(place * capacity, capacity)
        ]

        @pl.loop(1, group)
        def _(i):
            inplane(block, piece, i).start()

    barrier = pltpu.get_barrier_semaphore()

    @pl.loop(1, count)
    def _(i):
        pl.semaphore_signal(
            barrier, inc=1, device_id={"sp": lax.rem(me + i, count)}, device_id_type=MESH
        )

    pl.semaphore_signal(barrier, inc=1, device_id={"tp": other}, device_id_type=MESH)
    with jax.named_scope("slots"):
        names = route_ref[...].astype(f32)
        expert_row = lax.broadcasted_iota(jnp.int32, (count, tokens), 0).astype(f32)
        named = [jnp.where(expert_row == names[k : k + 1, :], 1.0, 0.0) for k in range(2)]
        earlier = lax.broadcasted_iota(jnp.int32, (tokens, tokens), 0) < lax.broadcasted_iota(
            jnp.int32, (tokens, tokens), 1
        )
        before = jnp.dot(
            (named[0] + named[1]).astype(bf16),
            jnp.where(earlier, 1.0, 0.0).astype(bf16),
            preferred_element_type=f32,
        )
        slots = [
            names[k : k + 1, :] * capacity + jnp.sum(named[k] * before, axis=0, keepdims=True)
            for k in range(2)
        ]
        info = jnp.concatenate(
            slots + [weight_ref[...], jnp.zeros((4, tokens), f32)], axis=0
        )
        small_ref[here] = info
        lanes = square_ref.shape[1]
        loads[2].wait()
        total = jnp.zeros((tokens, lanes), f32)
        for start in range(0, 2 * width, lanes):
            value = stream_ref[:, start : start + lanes].astype(f32)
            total = total + value * value
        square_ref[...] = total
        loads[0].wait()
        loads[1].wait()
    with jax.named_scope("greet"):
        pl.semaphore_wait(barrier, count)
    with jax.named_scope("own"):
        swap(0).start()

        @pl.loop(1, planes)
        def _(i):
            small(i).start()

        for i in range(3, 5):
            loads[i].wait()

        @pl.when(me < count - 1)
        def _():
            for i in range(2):
                rim_copy(i).start()

        for piece in range(2):
            for way in range(2):
                onward(way, here, piece)
        prepare(here, 0)
        for piece in range(2):
            pick(here, 0, piece)
        swap(0).wait_recv()
        total = square_ref[...] + square_other[...]
        inverse = lax.rsqrt(jnp.sum(total, axis=1, keepdims=True) / (4 * width) + EPSILON)
        for piece in range(2):
            cols = slice(piece * width, (piece + 1) * width)
            value = stream_ref[:, cols].astype(f32) * inverse * gain_ref[:, cols]
            column[here, 2 + piece] = value.astype(bf16)
        for piece in range(2, 4):
            for way in range(2):
                onward(way, here, piece)
        for piece in range(2, 4):
            pick(here, 0, piece)
        @pl.when(me == 0)
        def _():
            rim_ref[...] = jnp.zeros_like(rim_ref)

        spots = jnp.transpose(small_ref[here])
        slot = lax.broadcasted_iota(jnp.int32, pull_ref.shape, 1).astype(f32)
        hit = (slot == spots[:, 0:1]) | (slot == spots[:, 1:2])
        pull_ref[...] = jnp.where(hit, 1.0, 0.0).astype(bf16)

        @pl.loop(1, planes)
        def _(i):
            small_from(i).wait_recv()

        for i in range(5, 9):
            loads[i].wait()

    def arrive(step, piece):
        for way in range(2):
            block = here - step if way == 0 else here + step
            valid = (step < planes) & (block >= 0) & (block < planes)

            @pl.when(valid)
            def _():
                hop(way, block, piece).wait_recv()
                onward(way, block, piece)

        for way in range(2):
            block = here - step if way == 0 else here + step
            valid = (step < planes) & (block >= 0) & (block < planes)

            @pl.when(valid)
            def _():
                @pl.when(piece == 0)
                def _():
                    prepare(block, way)

                pick(block, way, piece)

    def gather(step, way):
        block = here - step + 2 * way * step
        valid = (block >= 0) & (block < planes) & ((way == 0) | (step > 0))

        @pl.when(valid)
        def _():
            @pl.loop(0, 4)
            def _(piece):
                @pl.loop(1, group)
                def _(i):
                    inplane(block, piece, i).wait_recv()

                cross(block, piece).start()

    def compute(step, way):
        block = here - step + 2 * way * step
        valid = (block >= 0) & (block < planes) & ((way == 0) | (step > 0))

        @pl.when(valid)
        def _():
            @pl.loop(0, 4)
            def _(piece):
                cross(block, piece).wait_recv()

            rows = span(block * bunch, bunch)
            gate_lin = jnp.zeros((bunch, gate_w.shape[1]), f32)
            up_lin = jnp.zeros((bunch, gate_w.shape[1]), f32)
            hidden_grad = jnp.zeros((bunch, gate_w.shape[1]), f32)
            for part in range(4):
                cols = slice(part * width, (part + 1) * width)
                inputs = rows_ref[1, part, rows]
                gate_lin += jnp.dot(inputs, gate_w[cols], preferred_element_type=f32)
                up_lin += jnp.dot(inputs, up_w[cols], preferred_element_type=f32)
                hidden_grad += contract_cols(rows_ref[0, part, rows], down_w[:, cols])
            sigmoid_gate = jax.nn.sigmoid(gate_lin)
            silu_gate = gate_lin * sigmoid_gate
            hidden_ref[rows] = (silu_gate * up_lin).astype(bf16)
            gate_pre = (
                hidden_grad * up_lin * sigmoid_gate * (1.0 + gate_lin * (1.0 - sigmoid_gate))
            ).astype(bf16)
            up_pre = (hidden_grad * silu_gate).astype(bf16)
            gate_pre_ref[rows] = gate_pre
            up_pre_ref[rows] = up_pre

            def partial(whose, half):
                spot = span((2 * whose + half) * width, width)
                value = contract_cols(gate_pre_ref[rows], gate_w[spot])
                value += contract_cols(up_pre_ref[rows], up_w[spot])
                return value.astype(bf16)

            for half in range(2):
                part_ref[block, :, half * width : (half + 1) * width] = partial(other, half)
                part_copy(block, half).start()
            for half in range(2):
                cols = slice(half * width, (half + 1) * width)
                mine = partial(side, half).astype(f32)
                part_copy(block, half).wait_recv()
                theirs = theirs_ref[block, :, cols].astype(f32)
                theirs_ref[block, :, cols] = (mine + theirs).astype(bf16)

    def written(i):
        mine, target = (
            (grad_ref, grad_hbm),
            (proj_out, proj_hbm_out),
            (u_out, u_hbm_out),
            (b_out, b_hbm_out),
            (c_out, c_hbm_out),
        )[i]
        return pltpu.make_async_copy(mine, target, finish.at[i])

    def stored(part):
        slot = lax.rem(part, 2)
        spot = span(part * width, width)
        return [
            pltpu.make_async_copy(stage_ref.at[slot, 0], gate_out.at[spot], store.at[slot, 0]),
            pltpu.make_async_copy(stage_ref.at[slot, 1], up_out.at[spot], store.at[slot, 1]),
            pltpu.make_async_copy(tall_ref.at[slot], down_out.at[:, spot], store.at[slot, 2]),
        ]

    def reply(step, way):
        block = here - step + 2 * way * step
        valid = (block >= 0) & (block < planes) & ((way == 0) | (step > 0))

        @pl.when(valid)
        def _():
            @pl.loop(0, group)
            def _(i):
                @pl.when(block * group + i != me)
                def _():
                    back(block, i).start()

                @pl.when(block * group + i == me)
                def _():
                    ret_ref[span(me * capacity, capacity)] = theirs_ref[
                        block, span(i * capacity, capacity)
                    ]

    def convolve():
        with jax.named_scope("conv"):

            @pl.when(me > 0)
            def _():
                for i in range(2):
                    rim_copy(i).wait_recv()

            gated = c_ref[...].astype(f32) * u_ref[...].astype(f32)
            rim_gated = rim_ref[1].astype(f32) * rim_ref[0].astype(f32)
            row = lax.broadcasted_iota(jnp.int32, gated.shape, 0)
            one = jnp.where(row == 0, rim_gated[rim - 1 : rim], pltpu.roll(gated, 1, 0))
            two = jnp.where(
                row == 0,
                rim_gated[rim - 2 : rim - 1],
                jnp.where(row == 1, rim_gated[rim - 1 : rim], pltpu.roll(gated, 2, 0)),
            )
            conv = taps_ref[0:1, :] * two + taps_ref[1:2, :] * one + taps_ref[2:3, :] * gated
            conv_ref[...] = conv
            mixed_value = (b_ref[...].astype(f32) * conv).astype(bf16)
            mixed_ref[...] = mixed_value
            near_ref[span(place * tokens, tokens)] = mixed_value

    inside = (here > 0) & (here < planes - 1)

    @pl.loop(1, planes + 1)
    def _(step):
        with jax.named_scope("arrive0"):

            @pl.loop(0, 2)
            def _(piece):
                arrive(step, piece)

        with jax.named_scope("gather"):

            @pl.loop(0, 2)
            def _(way):
                gather(step - 1, way)

        @pl.loop(0, 2)
        def _(way):
            with jax.named_scope("compute"):
                compute(step - 1, way)

        with jax.named_scope("arrive2"):

            @pl.loop(2, 4)
            def _(piece):
                arrive(step, piece)

        @pl.loop(0, 2)
        def _(way):
            reply(step - 1, way)

        @pl.when(step == 1)
        def _():
            convolve()

        @pl.when(step == jnp.where(inside, planes, 2))
        def _():
            @pl.loop(1, group)
            def _(i):
                mixed(i).start()

    loads[9].start()
    with jax.named_scope("wgrad"):

        @pl.loop(0, 4)
        def _(part):
            slot = lax.rem(part, 2)

            @pl.when(part >= 2)
            def _():
                for copy in stored(part - 2):
                    copy.wait()

            inputs = rows_ref[1, part]
            stage_ref[slot, 0] = contract_rows(inputs, gate_pre_ref[...])
            stage_ref[slot, 1] = contract_rows(inputs, up_pre_ref[...])
            tall_ref[slot] = contract_rows(hidden_ref[...], rows_ref[0, part])
            for copy in stored(part):
                copy.start()

    @pl.loop(0, planes)
    def _(turn):
        block = lax.rem(here + turn, planes)
        with jax.named_scope("returned"):

            @pl.loop(0, group)
            def _(i):
                @pl.when(block * group + i != me)
                def _():
                    back_from(block * group + i).wait_recv()

        with jax.named_scope("pull"):
            rows = span(block * bunch, bunch)
            value = jnp.dot(pull_ref[:, rows], ret_ref[rows], preferred_element_type=f32)

            @pl.when(turn == 0)
            def _():
                total_ref[...] = value

            @pl.when(turn > 0)
            def _():
                total_ref[...] += value

    with jax.named_scope("cross"):
        total = jnp.zeros((tokens, lanes), f32)
        for start in range(0, 2 * width, lanes):
            cols = slice(start, start + lanes)
            total += stream_ref[:, cols].astype(f32) * gain_ref[:, cols] * total_ref[:, cols]
        inner_ref[...] = total
        swap(1).start()
        square = jnp.sum(square_ref[...] + square_other[...], axis=1, keepdims=True)
        inverse = lax.rsqrt(square / (4 * width) + EPSILON)
        swap(1).wait_recv()
        inner = jnp.sum(inner_ref[...] + inner_other[...], axis=1, keepdims=True)
        pull_back = inverse * inverse * inverse * inner / (4 * width)
        for piece in range(2):
            cols = slice(piece * width, (piece + 1) * width)
            grad_ref[:, cols] = (
                column[here, piece].astype(f32)
                + inverse * gain_ref[:, cols] * total_ref[:, cols]
                - stream_ref[:, cols].astype(f32) * pull_back
            ).astype(bf16)
        swap(2).start()
        written(0).start()

    upper = here >= planes // 2
    base = lax.div(here * parts, planes)

    def turned(k):
        return lax.rem(base + parts + jnp.where(upper, 1 + k, parts - 1 - k), parts)

    with jax.named_scope("spread"):

        if not plain:
            features = 2 * width
            run = near * sliver
            for start in range(0, features, sliver):
                goal = lax.broadcasted_iota(jnp.int32, (features, sliver), 1) + start
                inner_goal = lax.rem(goal, run)
                origin = (
                    lax.div(inner_goal, depth) * group + lax.div(goal, run)
                ) * depth + lax.rem(inner_goal, depth)
                match = lax.broadcasted_iota(jnp.int32, (features, sliver), 0) == origin
                turn_ref[:, start : start + sliver] = jnp.dot(
                    grad_ref[...],
                    jnp.where(match, 1.0, 0.0).astype(bf16),
                    preferred_element_type=f32,
                ).astype(bf16)

        @pl.loop(0, parts)
        def _(k):
            part = turned(k)

            @pl.when(owned(part))
            def _():
                @pl.loop(0, group)
                def _(target):
                    @pl.when(target != place)
                    def _():
                        spread(target, part).start()

                block_ref[part, span(place * tokens, tokens)] = strip(place, part)[...]

    with jax.named_scope("mixer"):
        half = 2 * width
        loads[9].wait()
        mixer_grad = jnp.dot(
            grad_ref[...], gate_w[span(side * half, half)], preferred_element_type=f32
        )
        swap(2).wait_recv()
        mixer_grad += jnp.dot(
            grad_other[...], gate_w[span(other * half, half)], preferred_element_type=f32
        )
        delta = mixer_grad * b_ref[...].astype(f32)
        edge_ref[...] = delta[0 : edge_ref.shape[0]]

        @pl.when(me > 0)
        def _():
            edge_copy.start()

        b_out[...] = (mixer_grad * conv_ref[...]).astype(bf16)
        written(3).start()

    @pl.loop(1, group)
    def _(i):
        mixed(i).wait()

    @pl.loop(0, parts)
    def _(k):
        part = turned(k)
        with jax.named_scope("collect"):

            @pl.when(owned(part))
            def _():
                @pl.loop(0, group)
                def _(source):
                    @pl.when(source != place)
                    def _():
                        spread_from(source, part).wait_recv()

                hand(part).start()

            @pl.when(jnp.logical_not(owned(part)))
            def _():
                hand(part).wait_recv()

        with jax.named_scope("shares"):
            value = contract_rows(block_ref[part], near_ref[...])
            share_ref[part] = value.astype(bf16)
            for j in range(per_part):

                @pl.when(part * per_part + j != here)
                def _():
                    share(part, j).start()

                @pl.when(part * per_part + j == here)
                def _():
                    proj_out[...] = value[j * depth : (j + 1) * depth]

    with jax.named_scope("edge"):

        @pl.when(me == count - 1)
        def _():
            edge_next[...] = jnp.zeros_like(edge_next)

        @pl.when(me < count - 1)
        def _():
            edge_copy.wait_recv()

        row = lax.broadcasted_iota(jnp.int32, delta.shape, 0)
        one = jnp.where(
            row == tokens - 1, edge_next[0:1], pltpu.roll(delta, tokens - 1, 0)
        )
        two = jnp.where(
            row == tokens - 2,
            edge_next[0:1],
            jnp.where(row == tokens - 1, edge_next[1:2], pltpu.roll(delta, tokens - 2, 0)),
        )
        gated_grad = taps_ref[2:3, :] * delta + taps_ref[1:2, :] * one + taps_ref[0:1, :] * two
        u_out[...] = (gated_grad * c_ref[...].astype(f32)).astype(bf16)
        c_out[...] = (gated_grad * u_ref[...].astype(f32)).astype(bf16)
        written(2).start()
        written(4).start()

    for part in range(2, 4):
        for copy in stored(part):
            copy.wait()

    with jax.named_scope("final"):

        @pl.loop(1, planes)
        def _(i):
            source = lax.rem(here + i, planes)
            share_from(source).wait_recv()
            proj_out[...] += stack_ref[source].astype(f32)

    written(1).start()

    @pl.loop(0, planes)
    def _(block):
        @pl.loop(0, 4)
        def _(piece):
            for way in range(2):
                room = here < planes - 1 if way == 0 else here > 0
                mine = block <= here if way == 0 else block >= here

                @pl.when(room & mine)
                def _():
                    hop(way, block, piece).wait_send()

            cross(block, piece).wait_send()

            @pl.loop(1, group)
            def _(i):
                inplane(block, piece, i).wait_send()

        for half in range(2):
            part_copy(block, half).wait_send()

        @pl.loop(0, group)
        def _(i):
            @pl.when(block * group + i != me)
            def _():
                back(block, i).wait_send()

    @pl.loop(1, planes)
    def _(i):
        small(i).wait_send()

    @pl.when(me < count - 1)
    def _():
        for i in range(2):
            rim_copy(i).wait_send()

    @pl.when(me > 0)
    def _():
        edge_copy.wait_send()

    for i in range(3):
        swap(i).wait_send()

    @pl.loop(0, parts)
    def _(part):
        @pl.when(owned(part))
        def _():
            @pl.loop(0, group)
            def _(target):
                @pl.when(target != place)
                def _():
                    spread(target, part).wait_send()

            hand(part).wait_send()

        for j in range(per_part):

            @pl.when(part * per_part + j != here)
            def _():
                share(part, j).wait_send()

    for i in range(5):
        written(i).wait()


def local(
    stream,
    norm_gain,
    cotangent,
    route_weights,
    routes,
    conv_input,
    conv_bgate,
    conv_cgate,
    conv_taps,
    out_proj,
    gate_weight,
    up_weight,
    down_weight,
):
    count = lax.axis_size("sp")
    group = 2 ** ((count.bit_length() - 1) // 2)
    planes = count // group
    tokens, features = stream.shape
    width = features // 2
    channels = conv_input.shape[1]
    gate_shape, down_shape = gate_weight.shape[1:], down_weight.shape[1:]
    hidden = gate_shape[1]
    capacity = 2 * tokens * routes.shape[1] // count
    bunch = group * capacity
    slots = count * capacity
    depth = 2 * features // count
    sliver = max(128, depth)
    parts = planes * depth // sliver
    f32, bf16 = jnp.float32, jnp.bfloat16
    shape = jax.ShapeDtypeStruct
    outs = (
        shape(stream.shape, bf16),
        shape((depth, channels), f32),
        shape(conv_input.shape, bf16),
        shape(conv_input.shape, bf16),
        shape(conv_input.shape, bf16),
        shape(gate_shape, f32),
        shape(gate_shape, f32),
        shape(down_shape, f32),
    )
    vmem, hbm = pl.BlockSpec(memory_space=pltpu.VMEM), pl.BlockSpec(memory_space=pltpu.HBM)
    dma = pltpu.SemaphoreType.DMA
    results = pl.pallas_call(
        lambda *refs: layer_kernel(planes, group, *refs),
        out_shape=outs,
        in_specs=[hbm, vmem, hbm, vmem, vmem, hbm, hbm, hbm, vmem, hbm, hbm, hbm, hbm],
        out_specs=[hbm] * 8,
        scratch_shapes=[
            pltpu.VMEM((planes, 4, tokens, width), bf16),
            pltpu.VMEM((planes, 4, bunch, width), bf16),
            pltpu.VMEM((2, 4, slots, width), bf16),
            pltpu.VMEM(gate_shape, bf16),
            pltpu.VMEM(gate_shape, bf16),
            pltpu.VMEM(down_shape, bf16),
            pltpu.VMEM((slots, hidden), bf16),
            pltpu.VMEM((slots, hidden), bf16),
            pltpu.VMEM((slots, hidden), bf16),
            pltpu.VMEM((planes, bunch, features), bf16),
            pltpu.VMEM((planes, bunch, features), bf16),
            pltpu.VMEM((slots, features), bf16),
            pltpu.VMEM((tokens, features), bf16),
            pltpu.VMEM((tokens, channels), bf16),
            pltpu.VMEM((tokens, channels), bf16),
            pltpu.VMEM((tokens, channels), bf16),
            pltpu.VMEM((tokens, channels), f32),
            pltpu.VMEM((group * tokens, channels), bf16),
            pltpu.VMEM((2, 16, channels), bf16),
            pltpu.VMEM((tokens, channels), bf16),
            pltpu.VMEM((planes, 8, tokens), f32),
            pltpu.VMEM((tokens, 128), f32),
            pltpu.VMEM((tokens, 128), f32),
            pltpu.VMEM((tokens, 128), f32),
            pltpu.VMEM((tokens, 128), f32),
            pltpu.VMEM((2, bunch, tokens), bf16),
            pltpu.VMEM((2, bunch, 128), f32),
            pltpu.VMEM((tokens, slots), bf16),
            pltpu.VMEM((tokens, features), f32),
            pltpu.VMEM((tokens, features), bf16),
            pltpu.VMEM((parts, group * tokens, sliver), bf16),
            pltpu.VMEM((parts, sliver, channels), bf16),
            pltpu.VMEM((planes, depth, channels), bf16),
            pltpu.VMEM((8, channels), f32),
            pltpu.VMEM((8, channels), f32),
            pltpu.VMEM(stream.shape, bf16),
            pltpu.VMEM((depth, channels), f32),
            pltpu.VMEM(conv_input.shape, bf16),
            pltpu.VMEM(conv_input.shape, bf16),
            pltpu.VMEM(conv_input.shape, bf16),
            pltpu.VMEM(stream.shape if sliver > depth else (8, 128), bf16),
            pltpu.VMEM((2, 2, width, hidden), f32),
            pltpu.VMEM((2, hidden, width), f32),
            dma((10,)),
            dma((2, 3)),
            dma((5,)),
            dma((2, planes, 4)),
            dma((planes, 4)),
            dma((planes, 4, group)),
            dma((planes, 4, group)),
            dma((planes, 4)),
            dma((planes, 4)),
            dma((planes, 2)),
            dma((planes, 2)),
            dma((planes, group)),
            dma((count,)),
            dma((planes,)),
            dma((planes,)),
            dma((2,)),
            dma((2,)),
            dma((3,)),
            dma((3,)),
            dma((group,)),
            dma((group,)),
            dma((group, parts)),
            dma((group, parts)),
            dma((parts,)),
            dma((parts,)),
            dma((parts, planes // parts)),
            dma((planes,)),
            dma,
            dma,
        ],
        compiler_params=pltpu.CompilerParams(
            collective_id=0, has_side_effects=True, vmem_limit_bytes=VMEM_LIMIT
        ),
        name="layer",
    )(
        stream,
        norm_gain[None, :],
        cotangent,
        route_weights.T,
        routes.T,
        conv_input,
        conv_bgate,
        conv_cgate,
        conv_taps,
        out_proj,
        gate_weight[0],
        up_weight[0],
        down_weight[0],
    )
    return results[:5] + tuple(value[None] for value in results[5:])


def solution(mesh):
    return jax.shard_map(
        local,
        mesh=mesh,
        in_specs=(
            P("sp", "tp"),
            P("tp"),
            P("sp", "tp"),
            P("sp", None),
            P("sp", None),
            P("sp", "tp"),
            P("sp", "tp"),
            P("sp", "tp"),
            P(None, "tp"),
            P(None, "tp"),
            P("sp", None, "tp"),
            P("sp", None, "tp"),
            P("sp", "tp", None),
        ),
        out_specs=(
            P("sp", "tp"),
            P("sp", "tp"),
            P("sp", "tp"),
            P("sp", "tp"),
            P("sp", "tp"),
            P("sp", None, "tp"),
            P("sp", None, "tp"),
            P("sp", "tp", None),
        ),
        check_vma=False,
    )
```

```python
import jax
import jax.numpy as jnp
from jax import lax
from jax.experimental import pallas as pl
from jax.experimental.pallas import tpu as pltpu
from jax.sharding import PartitionSpec as P

EPSILON = 1e-06


def contract_rows(left, right):
    return lax.dot_general(
        left, right, (((0,), (0,)), ((), ())), preferred_element_type=jnp.float32
    )


def contract_cols(left, right):
    return lax.dot_general(
        left, right, (((1,), (1,)), ((), ())), preferred_element_type=jnp.float32
    )


MESH = pl.DeviceIdType.MESH
MIB = 2**20


def layer_kernel(
    planes,
    group,
    stream_hbm,
    gain_hbm,
    cot_hbm,
    weight_hbm,
    route_hbm,
    u_hbm,
    b_hbm,
    c_hbm,
    taps_hbm,
    proj_hbm,
    gate_hbm,
    up_hbm,
    down_hbm,
    grad_ref,
    proj_out,
    u_out,
    b_out,
    c_out,
    *rest,
):
    pieces = rest[:12]
    (
        gain_ref,
        weight_ref,
        route_ref,
        taps_ref,
        column,
        outgoing,
        rows_ref,
        gate_w,
        up_w,
        down_w,
        hidden_ref,
        gate_pre_ref,
        up_pre_ref,
        part_ref,
        theirs_ref,
        ret_ref,
            u_ref,
        b_ref,
        c_ref,
            near_ref,
        rim_ref,
        small_ref,
        square_ref,
        square_other,
        inner_ref,
        inner_other,
        select_ref,
            spots_ref,
        total_ref,
        grad_other,
        block_ref,
            stack_ref,
        edge_ref,
        edge_next,
        turn_ref,
        load,
        hop_send,
        hop_recv,
        plane_send,
        plane_recv,
        cross_send,
        cross_recv,
        part_send,
        part_recv,
        back_send,
        back_recv,
        small_send,
        small_recv,
        rim_send,
        rim_recv,
        side_send,
        side_recv,
        mixed_send,
        mixed_recv,
        spread_send,
        spread_recv,
        pass_send,
        pass_recv,
        share_send,
        share_recv,
        edge_send,
        edge_recv,
    ) = rest[12:]
    count = planes * group
    me = lax.axis_index("sp")
    side = lax.axis_index("tp")
    other = 1 - side
    here = lax.div(me, group)
    place = lax.rem(me, group)
    tokens = grad_ref.shape[0]
    width = column.shape[3]
    bunch = outgoing.shape[2]
    capacity = bunch // group
    f32, bf16 = jnp.float32, jnp.bfloat16

    def local(i, source, target):
        return pltpu.make_async_copy(source, target, load.at[i])

    def remote(source, target, sent, received, **peer):
        return pltpu.make_async_remote_copy(
            src_ref=source,
            dst_ref=target,
            send_sem=sent,
            recv_sem=received,
            device_id=peer,
            device_id_type=MESH,
        )

    loads = [
        local(0, cot_hbm.at[0, :, 0:width], column.at[here, 0]),
        local(1, cot_hbm.at[0, :, width : 2 * width], column.at[here, 1]),
        local(2, stream_hbm.at[0], grad_ref),
        local(3, u_hbm.at[0], u_ref),
        local(4, c_hbm.at[0], c_ref),
        local(5, b_hbm.at[0], b_ref),
        local(6, gate_hbm.at[0], gate_w),
        local(7, up_hbm.at[0], up_w),
        local(8, down_hbm.at[0], down_w),
        local(9, proj_hbm.at[0], gate_w),
        local(10, route_hbm, route_ref),
        local(11, weight_hbm, weight_ref),
        local(12, gain_hbm, gain_ref),
        local(13, taps_hbm, taps_ref),
    ]
    for copy in loads[10:] + loads[:9]:
        copy.start()

    def hop(way, block, piece):
        spot = column.at[block, piece]
        return remote(
            spot,
            spot,
            hop_send.at[way, block, piece],
            hop_recv.at[block, piece],
            sp=me + (1 - 2 * way) * group,
        )

    def onward(way, block, piece):
        room = here < planes - 1 if way == 0 else here > 0

        @pl.when(room)
        def _():
            hop(way, block, piece).start()

    def small(i):
        return remote(
            small_ref.at[here],
            small_ref.at[here],
            small_send.at[i],
            small_recv.at[i],
            sp=lax.rem(here + i, planes) * group + place,
        )

    def small_from(i):
        return remote(
            small_ref.at[here],
            small_ref.at[lax.rem(here + planes - i, planes)],
            small_send.at[i],
            small_recv.at[i],
            sp=lax.rem(here + i, planes) * group + place,
        )

    def stripe(piece):
        return lax.div(piece, 2), 2 * side + lax.rem(piece, 2)

    def span(start, size):
        return pl.ds(pl.multiple_of(start, size), size)

    def inplane(block, piece, i):
        target = lax.rem(place + i, group)
        kind, part = stripe(piece)
        return remote(
            outgoing.at[block, piece, span(target * capacity, capacity)],
            rows_ref.at[kind, part, span(block * bunch + place * capacity, capacity)],
            plane_send.at[block, piece, i],
            plane_recv.at[block, piece, i],
            sp=here * group + target,
        )

    def cross(block, piece):
        kind, part = stripe(piece)
        spot = rows_ref.at[kind, part, span(block * bunch, bunch)]
        return remote(
            spot, spot, cross_send.at[block, piece], cross_recv.at[block, piece], tp=other
        )

    def part_copy(block, half):
        return remote(
            part_ref.at[:, half * width : (half + 1) * width],
            theirs_ref.at[block, :, half * width : (half + 1) * width],
            part_send.at[block, half],
            part_recv.at[block, half],
            tp=other,
        )

    def back(block, i):
        return remote(
            theirs_ref.at[block, span(i * capacity, capacity)],
            ret_ref.at[span(me * capacity, capacity)],
            back_send.at[block, i],
            back_recv.at[me],
            sp=block * group + i,
        )

    def back_from(source):
        return remote(
            theirs_ref.at[0, pl.ds(0, capacity)],
            ret_ref.at[span(source * capacity, capacity)],
            back_send.at[0, 0],
            back_recv.at[source],
            sp=source,
        )

    rim = rim_ref.shape[1]

    def rim_copy(i):
        source = (u_ref, c_ref)[i]
        return remote(
            source.at[tokens - rim : tokens],
            rim_ref.at[i],
            rim_send.at[i],
            rim_recv.at[i],
            sp=me + 1,
        )

    def mixed(i):
        return remote(
            near_ref.at[span(place * tokens, tokens)],
            near_ref.at[span(place * tokens, tokens)],
            mixed_send.at[i],
            mixed_recv.at[i],
            sp=here * group + lax.rem(place + i, group),
        )

    def swap(i):
        mine, yours = (
            (square_ref, square_other),
            (inner_ref, inner_other),
            (grad_ref, grad_other),
        )[i]
        return remote(mine, yours, side_send.at[i], side_recv.at[i], tp=other)

    parts, sliver = block_ref.shape[0], block_ref.shape[2]
    per_part = planes // parts
    near = parts // 2
    depth = proj_out.shape[0]
    plain = per_part == 1

    def owned(part):
        return lax.div(part, near) == side

    def strip(target, part):
        if plain:
            start = ((part - side * near) * group + target) * sliver
        else:
            start = (target * near + part - side * near) * sliver
        return (grad_ref if plain else turn_ref).at[:, span(start, sliver)]

    def spread(target, part):
        return remote(
            strip(target, part),
            block_ref.at[part, span(place * tokens, tokens)],
            spread_send.at[target, part],
            spread_recv.at[place, part],
            sp=here * group + target,
        )

    def spread_from(source, part):
        return remote(
            grad_ref.at[:, pl.ds(0, sliver)],
            block_ref.at[part, span(source * tokens, tokens)],
            spread_send.at[source, part],
            spread_recv.at[source, part],
            sp=here * group + source,
        )

    def hand(part):
        spot = block_ref.at[part]
        return remote(spot, spot, pass_send.at[part], pass_recv.at[part], tp=other)

    def share(part, j):
        target = part * per_part + j
        return remote(
            gate_pre_ref.at[span(part * sliver + j * depth, depth)],
            stack_ref.at[here],
            share_send.at[part, j],
            share_recv.at[here],
            sp=target * group + place,
        )

    def share_from(source):
        return remote(
            gate_pre_ref.at[pl.ds(0, depth)],
            stack_ref.at[source],
            share_send.at[0, 0],
            share_recv.at[source],
            sp=source * group + place,
        )

    edge_copy = remote(edge_ref, edge_next, edge_send, edge_recv, sp=me - 1)


    def places(block):
        wanted = lax.broadcasted_iota(jnp.int32, (bunch, tokens), 0) + here * bunch
        wanted = wanted.astype(f32)
        return wanted == small_ref[block, 0:1, :], wanted == small_ref[block, 1:2, :]

    def prepare(block, way):
        first, second = places(block)
        select_ref[way] = jnp.where(first | second, 1.0, 0.0).astype(bf16)

    def pick(block, way, piece):
        chosen = jnp.dot(select_ref[way], column[block, piece], preferred_element_type=f32)

        first, second = places(block)
        weight = jnp.where(first, small_ref[block, 2:3, :], 0.0)
        weight += jnp.where(second, small_ref[block, 3:4, :], 0.0)
        scale = jnp.where(piece < 2, jnp.sum(weight, axis=1, keepdims=True), 1.0)
        outgoing[block, piece] = (chosen * scale).astype(bf16)
        kind, part = stripe(piece)
        rows_ref[kind, part, span(block * bunch + place * capacity, capacity)] = outgoing[
            block, piece, span(place * capacity, capacity)
        ]

        @pl.loop(1, group)
        def _(i):
            inplane(block, piece, i).start()

    barrier = pltpu.get_barrier_semaphore()

    @pl.loop(1, count)
    def _(i):
        pl.semaphore_signal(
            barrier, inc=1, device_id={"sp": lax.rem(me + i, count)}, device_id_type=MESH
        )

    pl.semaphore_signal(barrier, inc=1, device_id={"tp": other}, device_id_type=MESH)
    with jax.named_scope("slots"):
        for i in range(10, 14):
            loads[i].wait()
        names = route_ref[...].astype(f32)
        expert_row = lax.broadcasted_iota(jnp.int32, (count, tokens), 0).astype(f32)
        named = [jnp.where(expert_row == names[k : k + 1, :], 1.0, 0.0) for k in range(2)]
        earlier = lax.broadcasted_iota(jnp.int32, (tokens, tokens), 0) < lax.broadcasted_iota(
            jnp.int32, (tokens, tokens), 1
        )
        before = jnp.dot(
            (named[0] + named[1]).astype(bf16),
            jnp.where(earlier, 1.0, 0.0).astype(bf16),
            preferred_element_type=f32,
        )
        slots = [
            names[k : k + 1, :] * capacity + jnp.sum(named[k] * before, axis=0, keepdims=True)
            for k in range(2)
        ]
        info = jnp.concatenate(
            slots + [weight_ref[...], jnp.zeros((4, tokens), f32)], axis=0
        )
        small_ref[here] = info
        lanes = square_ref.shape[1]
        loads[2].wait()
        total = jnp.zeros((tokens, lanes), f32)
        for start in range(0, 2 * width, lanes):
            value = grad_ref[:, start : start + lanes].astype(f32)
            total = total + value * value
        square_ref[...] = total
        loads[0].wait()
        loads[1].wait()
    with jax.named_scope("greet"):
        pl.semaphore_wait(barrier, count)
    with jax.named_scope("own"):
        swap(0).start()

        @pl.loop(1, planes)
        def _(i):
            small(i).start()

        for i in range(3, 5):
            loads[i].wait()

        @pl.when(me < count - 1)
        def _():
            for i in range(2):
                rim_copy(i).start()

        for piece in range(2):
            for way in range(2):
                onward(way, here, piece)
        prepare(here, 0)
        for piece in range(2):
            pick(here, 0, jnp.int32(piece))
        swap(0).wait_recv()
        total = square_ref[...] + square_other[...]
        inverse = lax.rsqrt(jnp.sum(total, axis=1, keepdims=True) / (4 * width) + EPSILON)
        for piece in range(2):
            cols = slice(piece * width, (piece + 1) * width)
            value = grad_ref[:, cols].astype(f32) * inverse * gain_ref[:, cols]
            column[here, 2 + piece] = value.astype(bf16)
        for piece in range(2, 4):
            for way in range(2):
                onward(way, here, piece)
        for piece in range(2, 4):
            pick(here, 0, jnp.int32(piece))
        @pl.when(me == 0)
        def _():
            rim_ref[...] = jnp.zeros_like(rim_ref)

        spots_ref[...] = jnp.transpose(small_ref[here])

        @pl.loop(1, planes)
        def _(i):
            small_from(i).wait_recv()

        for i in range(5, 9):
            loads[i].wait()

    def arrive(step, piece):
        for way in range(2):
            block = here - step if way == 0 else here + step
            valid = (step < planes) & (block >= 0) & (block < planes)

            @pl.when(valid)
            def _():
                hop(way, block, piece).wait_recv()
                onward(way, block, piece)

        for way in range(2):
            block = here - step if way == 0 else here + step
            valid = (step < planes) & (block >= 0) & (block < planes)

            @pl.when(valid)
            def _():
                @pl.when(piece == 0)
                def _():
                    prepare(block, way)

                pick(block, way, piece)

    def collect(block, piece):
        @pl.loop(1, group)
        def _(i):
            inplane(block, piece, i).wait_recv()

        cross(block, piece).start()

    def gather(step, way):
        block = here - step + 2 * way * step
        valid = (block >= 0) & (block < planes) & ((way == 0) | (step > 0))

        @pl.when(valid)
        def _():
            @pl.loop(0, 3)
            def _(piece):
                collect(block, piece)

    def compute(step, way):
        block = here - step + 2 * way * step
        valid = (block >= 0) & (block < planes) & ((way == 0) | (step > 0))

        @pl.when(valid)
        def _():
            rows = span(block * bunch, bunch)
            gate_lin = jnp.zeros((bunch, gate_w.shape[1]), f32)
            up_lin = jnp.zeros((bunch, gate_w.shape[1]), f32)
            hidden_grad = jnp.zeros((bunch, gate_w.shape[1]), f32)
            for piece in range(2):
                cross(block, piece).wait_recv()
            for part in range(4):
                cols = slice(part * width, (part + 1) * width)
                hidden_grad += contract_cols(rows_ref[0, part, rows], down_w[:, cols])
            for piece in range(2, 4):
                if piece == 3:
                    collect(block, piece)
                cross(block, piece).wait_recv()
                for part in range(piece - 2, 4, 2):
                    cols = slice(part * width, (part + 1) * width)
                    inputs = rows_ref[1, part, rows]
                    gate_lin += jnp.dot(inputs, gate_w[cols], preferred_element_type=f32)
                    up_lin += jnp.dot(inputs, up_w[cols], preferred_element_type=f32)
            sigmoid_gate = jax.nn.sigmoid(gate_lin)
            silu_gate = gate_lin * sigmoid_gate
            hidden_ref[rows] = (silu_gate * up_lin).astype(bf16)
            gate_pre = (
                hidden_grad * up_lin * sigmoid_gate * (1.0 + gate_lin * (1.0 - sigmoid_gate))
            ).astype(bf16)
            up_pre = (hidden_grad * silu_gate).astype(bf16)
            gate_pre_ref[rows] = gate_pre
            up_pre_ref[rows] = up_pre

            def partial(whose, half):
                spot = span((2 * whose + half) * width, width)
                value = contract_cols(gate_pre_ref[rows], gate_w[spot])
                value += contract_cols(up_pre_ref[rows], up_w[spot])
                return value.astype(bf16)

            for half in range(2):
                part_ref[:, half * width : (half + 1) * width] = partial(other, half)
                part_copy(block, half).start()
            for half in range(2):
                cols = slice(half * width, (half + 1) * width)
                mine = partial(side, half).astype(f32)
                part_copy(block, half).wait_recv()
                theirs = theirs_ref[block, :, cols].astype(f32)
                theirs_ref[block, :, cols] = (mine + theirs).astype(bf16)
            for half in range(2):
                part_copy(block, half).wait_send()

    def reply(step, way):
        block = here - step + 2 * way * step
        valid = (block >= 0) & (block < planes) & ((way == 0) | (step > 0))

        @pl.when(valid)
        def _():
            @pl.loop(0, group)
            def _(turn):
                i = lax.rem(place + turn, group)

                @pl.when(block * group + i != me)
                def _():
                    back(block, i).start()

                @pl.when(block * group + i == me)
                def _():
                    ret_ref[span(me * capacity, capacity)] = theirs_ref[
                        block, span(i * capacity, capacity)
                    ]

    def convolve():
        gated = c_ref[...].astype(f32) * u_ref[...].astype(f32)
        rim_gated = rim_ref[1].astype(f32) * rim_ref[0].astype(f32)
        row = lax.broadcasted_iota(jnp.int32, gated.shape, 0)
        one = jnp.where(row == 0, rim_gated[rim - 1 : rim], pltpu.roll(gated, 1, 0))
        two = jnp.where(
            row == 0,
            rim_gated[rim - 2 : rim - 1],
            jnp.where(row == 1, rim_gated[rim - 1 : rim], pltpu.roll(gated, 2, 0)),
        )
        conv = taps_ref[0:1, :] * two + taps_ref[1:2, :] * one + taps_ref[2:3, :] * gated
        return conv

    inside = (here > 0) & (here < planes - 1)

    @pl.loop(1, planes + 1)
    def _(step):
        with jax.named_scope("arrive0"):

            @pl.loop(0, 2)
            def _(piece):
                arrive(step, piece)

        with jax.named_scope("gather"):

            @pl.loop(0, 2)
            def _(way):
                gather(step - 1, way)

        @pl.loop(0, 2)
        def _(way):
            with jax.named_scope("compute"):
                compute(step - 1, way)

        with jax.named_scope("arrive2"):

            @pl.loop(2, 4)
            def _(piece):
                arrive(step, piece)

        @pl.loop(0, 2)
        def _(way):
            reply(step - 1, way)

        @pl.when(step == 1)
        def _():
            @pl.when(me > 0)
            def _():
                for i in range(2):
                    rim_copy(i).wait_recv()

            mixed_value = b_ref[...].astype(f32) * convolve()
            near_ref[span(place * tokens, tokens)] = mixed_value.astype(bf16)

        @pl.when(step == jnp.where(inside, planes, 2))
        def _():
            @pl.loop(1, group)
            def _(i):
                mixed(i).start()

    loads[9].start()
    with jax.named_scope("wgrad"):

        for part in range(4):
            inputs = rows_ref[1, part]
            pieces[part][...] = contract_rows(inputs, gate_pre_ref[...])
            pieces[4 + part][...] = contract_rows(inputs, up_pre_ref[...])
            pieces[8 + part][...] = contract_rows(hidden_ref[...], rows_ref[0, part])

    @pl.loop(0, planes)
    def _(block):
        @pl.loop(0, 4)
        def _(piece):
            for way in range(2):
                room = here < planes - 1 if way == 0 else here > 0
                mine = block <= here if way == 0 else block >= here

                @pl.when(room & mine)
                def _():
                    hop(way, block, piece).wait_send()

            cross(block, piece).wait_send()

            @pl.loop(1, group)
            def _(i):
                inplane(block, piece, i).wait_send()

    @pl.loop(1, planes)
    def _(i):
        small(i).wait_send()

    @pl.when(me < count - 1)
    def _():
        for i in range(2):
            rim_copy(i).wait_send()

    swap(0).wait_send()

    @pl.loop(0, planes)
    def _(turn):
        block = lax.rem(here + turn, planes)
        with jax.named_scope("returned"):

            @pl.loop(0, group)
            def _(i):
                @pl.when(block * group + i != me)
                def _():
                    back_from(block * group + i).wait_recv()

        with jax.named_scope("pull"):
            rows = span(block * bunch, bunch)
            slot = lax.broadcasted_iota(jnp.int32, (tokens, bunch), 1) + block * bunch
            slot = slot.astype(f32)
            hit = (slot == spots_ref[:, 0:1]) | (slot == spots_ref[:, 1:2])
            pull = jnp.where(hit, 1.0, 0.0).astype(bf16)
            value = jnp.dot(pull, ret_ref[rows], preferred_element_type=f32)

            @pl.when(turn == 0)
            def _():
                total_ref[...] = value

            @pl.when(turn > 0)
            def _():
                total_ref[...] += value

    with jax.named_scope("cross"):
        total = jnp.zeros((tokens, lanes), f32)
        for start in range(0, 2 * width, lanes):
            cols = slice(start, start + lanes)
            total += grad_ref[:, cols].astype(f32) * gain_ref[:, cols] * total_ref[:, cols]
        inner_ref[...] = total
        swap(1).start()
        square = jnp.sum(square_ref[...] + square_other[...], axis=1, keepdims=True)
        inverse = lax.rsqrt(square / (4 * width) + EPSILON)
        swap(1).wait_recv()
        inner = jnp.sum(inner_ref[...] + inner_other[...], axis=1, keepdims=True)
        pull_back = inverse * inverse * inverse * inner / (4 * width)
        for piece in range(2):
            cols = slice(piece * width, (piece + 1) * width)
            grad_ref[:, cols] = (
                column[here, piece].astype(f32)
                + inverse * gain_ref[:, cols] * total_ref[:, cols]
                - grad_ref[:, cols].astype(f32) * pull_back
            ).astype(bf16)
        swap(2).start()

    upper = here >= planes // 2
    base = lax.div(here * parts, planes)

    def turned(k):
        return lax.rem(base + parts + jnp.where(upper, 1 + k, parts - 1 - k), parts)

    with jax.named_scope("spread"):

        if not plain:
            features = 2 * width
            run = near * sliver
            for start in range(0, features, sliver):
                goal = lax.broadcasted_iota(jnp.int32, (features, sliver), 1) + start
                inner_goal = lax.rem(goal, run)
                origin = (
                    lax.div(inner_goal, depth) * group + lax.div(goal, run)
                ) * depth + lax.rem(inner_goal, depth)
                match = lax.broadcasted_iota(jnp.int32, (features, sliver), 0) == origin
                turn_ref[:, start : start + sliver] = jnp.dot(
                    grad_ref[...],
                    jnp.where(match, 1.0, 0.0).astype(bf16),
                    preferred_element_type=f32,
                ).astype(bf16)

        @pl.loop(0, parts)
        def _(k):
            part = turned(k)

            @pl.when(owned(part))
            def _():
                @pl.loop(0, group)
                def _(target):
                    @pl.when(target != place)
                    def _():
                        spread(target, part).start()

                block_ref[part, span(place * tokens, tokens)] = strip(place, part)[...]

    with jax.named_scope("mixer"):
        half = 2 * width
        loads[9].wait()
        mixer_grad = jnp.dot(
            grad_ref[...], gate_w[span(side * half, half)], preferred_element_type=f32
        )
        swap(2).wait_recv()
        mixer_grad += jnp.dot(
            grad_other[...], gate_w[span(other * half, half)], preferred_element_type=f32
        )
        delta = mixer_grad * b_ref[...].astype(f32)
        edge_ref[...] = delta[0 : edge_ref.shape[0]]

        @pl.when(me > 0)
        def _():
            edge_copy.start()

        b_out[...] = (mixer_grad * convolve()).astype(bf16)

    @pl.loop(1, group)
    def _(i):
        mixed(i).wait()

    @pl.loop(0, parts)
    def _(k):
        part = turned(k)
        with jax.named_scope("collect"):

            @pl.when(owned(part))
            def _():
                @pl.loop(0, group)
                def _(source):
                    @pl.when(source != place)
                    def _():
                        spread_from(source, part).wait_recv()

                hand(part).start()

            @pl.when(jnp.logical_not(owned(part)))
            def _():
                hand(part).wait_recv()

        with jax.named_scope("shares"):
            value = contract_rows(block_ref[part], near_ref[...])
            gate_pre_ref[span(part * sliver, sliver)] = value.astype(bf16)
            for j in range(per_part):

                @pl.when(part * per_part + j != here)
                def _():
                    share(part, j).start()

                @pl.when(part * per_part + j == here)
                def _():
                    proj_out[...] = value[j * depth : (j + 1) * depth]

    with jax.named_scope("edge"):

        @pl.when(me == count - 1)
        def _():
            edge_next[...] = jnp.zeros_like(edge_next)

        @pl.when(me < count - 1)
        def _():
            edge_copy.wait_recv()

        row = lax.broadcasted_iota(jnp.int32, delta.shape, 0)
        one = jnp.where(
            row == tokens - 1, edge_next[0:1], pltpu.roll(delta, tokens - 1, 0)
        )
        two = jnp.where(
            row == tokens - 2,
            edge_next[0:1],
            jnp.where(row == tokens - 1, edge_next[1:2], pltpu.roll(delta, tokens - 2, 0)),
        )
        gated_grad = taps_ref[2:3, :] * delta + taps_ref[1:2, :] * one + taps_ref[0:1, :] * two
        u_out[...] = (gated_grad * c_ref[...].astype(f32)).astype(bf16)
        c_out[...] = (gated_grad * u_ref[...].astype(f32)).astype(bf16)

    @pl.loop(0, planes)
    def _(block):
        @pl.loop(0, group)
        def _(i):
            @pl.when(block * group + i != me)
            def _():
                back(block, i).wait_send()

    @pl.when(me > 0)
    def _():
        edge_copy.wait_send()

    for i in range(1, 3):
        swap(i).wait_send()

    @pl.loop(0, parts)
    def _(part):
        @pl.when(owned(part))
        def _():
            @pl.loop(0, group)
            def _(target):
                @pl.when(target != place)
                def _():
                    spread(target, part).wait_send()

            hand(part).wait_send()

    with jax.named_scope("final"):

        @pl.loop(1, planes)
        def _(i):
            source = lax.rem(here + i, planes)
            share_from(source).wait_recv()
            proj_out[...] += stack_ref[source].astype(f32)

    @pl.loop(0, parts)
    def _(part):
        for j in range(per_part):

            @pl.when(part * per_part + j != here)
            def _():
                share(part, j).wait_send()


def store_kernel(*refs):
    sources, targets, sems = refs[:17], refs[17:25], refs[25]
    copies = []
    for i in range(17):
        if i < 5:
            target = targets[i]
        else:
            which, part = (i - 5) // 4, (i - 5) % 4
            rows, cols = sources[i].shape
            target = targets[5 + which]
            if which < 2:
                target = target.at[pl.ds(part * rows, rows)]
            else:
                target = target.at[:, pl.ds(part * cols, cols)]
        copies.append(pltpu.make_async_copy(sources[i], target, sems.at[i]))
    for copy in copies:
        copy.start()
    for copy in copies:
        copy.wait()


def pinned(value):
    return pltpu.with_memory_space_constraint(value, pltpu.HBM)


def local(
    stream,
    norm_gain,
    cotangent,
    route_weights,
    routes,
    conv_input,
    conv_bgate,
    conv_cgate,
    conv_taps,
    out_proj,
    gate_weight,
    up_weight,
    down_weight,
):
    count = lax.axis_size("sp")
    group = 2 ** ((count.bit_length() - 1) // 2)
    planes = count // group
    tokens, features = stream.shape
    width = features // 2
    channels = conv_input.shape[1]
    gate_shape, down_shape = gate_weight.shape[1:], down_weight.shape[1:]
    hidden = gate_shape[1]
    capacity = 2 * tokens * routes.shape[1] // count
    bunch = group * capacity
    slots = count * capacity
    grant = 38 * MIB + 2 * planes * tokens * features * 2
    depth = 2 * features // count
    sliver = max(128, depth)
    parts = planes * depth // sliver
    f32, bf16 = jnp.float32, jnp.bfloat16
    shape = jax.ShapeDtypeStruct
    outs = (
        shape(stream.shape, bf16),
        shape((depth, channels), f32),
        shape(conv_input.shape, bf16),
        shape(conv_input.shape, bf16),
        shape(conv_input.shape, bf16),
        shape(gate_shape, f32),
        shape(gate_shape, f32),
        shape(down_shape, f32),
    )
    vmem, hbm = pl.BlockSpec(memory_space=pltpu.VMEM), pl.BlockSpec(memory_space=pltpu.HBM)
    dma = pltpu.SemaphoreType.DMA
    results = pl.pallas_call(
        lambda *refs: layer_kernel(planes, group, *refs),
        out_shape=tuple(pltpu.VMEM(out.shape, out.dtype) for out in outs[:5])
        + (pltpu.VMEM((width, hidden), f32),) * 8
        + (pltpu.VMEM((hidden, width), f32),) * 4,
        in_specs=[hbm] * 13,
        out_specs=[vmem] * 17,
        scratch_shapes=[
            pltpu.VMEM((1, features), f32),
            pltpu.VMEM(route_weights.shape[::-1], f32),
            pltpu.VMEM(routes.shape[::-1], jnp.int32),
            pltpu.VMEM(conv_taps.shape, f32),
            pltpu.VMEM((planes, 4, tokens, width), bf16),
            pltpu.VMEM((planes, 4, bunch, width), bf16),
            pltpu.VMEM((2, 4, slots, width), bf16),
            pltpu.VMEM(gate_shape, bf16),
            pltpu.VMEM(gate_shape, bf16),
            pltpu.VMEM(down_shape, bf16),
            pltpu.VMEM((slots, hidden), bf16),
            pltpu.VMEM((slots, hidden), bf16),
            pltpu.VMEM((slots, hidden), bf16),
            pltpu.VMEM((bunch, features), bf16),
            pltpu.VMEM((planes, bunch, features), bf16),
            pltpu.VMEM((slots, features), bf16),
            pltpu.VMEM((tokens, channels), bf16),
            pltpu.VMEM((tokens, channels), bf16),
            pltpu.VMEM((tokens, channels), bf16),
            pltpu.VMEM((group * tokens, channels), bf16),
            pltpu.VMEM((2, 16, channels), bf16),
            pltpu.VMEM((planes, 8, tokens), f32),
            pltpu.VMEM((tokens, 128), f32),
            pltpu.VMEM((tokens, 128), f32),
            pltpu.VMEM((tokens, 128), f32),
            pltpu.VMEM((tokens, 128), f32),
            pltpu.VMEM((2, bunch, tokens), bf16),
            pltpu.VMEM((tokens, 8), f32),
            pltpu.VMEM((tokens, features), f32),
            pltpu.VMEM((tokens, features), bf16),
            pltpu.VMEM((parts, group * tokens, sliver), bf16),
            pltpu.VMEM((planes, depth, channels), bf16),
            pltpu.VMEM((8, channels), f32),
            pltpu.VMEM((8, channels), f32),
            pltpu.VMEM(stream.shape if sliver > depth else (8, 128), bf16),
            dma((14,)),
            dma((2, planes, 4)),
            dma((planes, 4)),
            dma((planes, 4, group)),
            dma((planes, 4, group)),
            dma((planes, 4)),
            dma((planes, 4)),
            dma((planes, 2)),
            dma((planes, 2)),
            dma((planes, group)),
            dma((count,)),
            dma((planes,)),
            dma((planes,)),
            dma((2,)),
            dma((2,)),
            dma((3,)),
            dma((3,)),
            dma((group,)),
            dma((group,)),
            dma((group, parts)),
            dma((group, parts)),
            dma((parts,)),
            dma((parts,)),
            dma((parts, planes // parts)),
            dma((planes,)),
            dma,
            dma,
        ],
        compiler_params=pltpu.CompilerParams(
            collective_id=0, has_side_effects=True, vmem_limit_bytes=grant
        ),
        name="layer",
    )(
        pinned(stream[None]),
        pinned(norm_gain[None, :]),
        pinned(cotangent[None]),
        pinned(route_weights.T),
        pinned(routes.T),
        pinned(conv_input[None]),
        pinned(conv_bgate[None]),
        pinned(conv_cgate[None]),
        pinned(conv_taps),
        pinned(out_proj[None]),
        pinned(gate_weight),
        pinned(up_weight),
        pinned(down_weight),
    )
    results = pl.pallas_call(
        store_kernel,
        out_shape=outs,
        in_specs=[vmem] * 17,
        out_specs=[hbm] * 8,
        scratch_shapes=[dma((17,))],
        compiler_params=pltpu.CompilerParams(vmem_limit_bytes=2**20),
        name="store",
    )(*results)
    return tuple(results[:5]) + tuple(value[None] for value in results[5:])


def solution(mesh):
    return jax.shard_map(
        local,
        mesh=mesh,
        in_specs=(
            P("sp", "tp"),
            P("tp"),
            P("sp", "tp"),
            P("sp", None),
            P("sp", None),
            P("sp", "tp"),
            P("sp", "tp"),
            P("sp", "tp"),
            P(None, "tp"),
            P(None, "tp"),
            P("sp", None, "tp"),
            P("sp", None, "tp"),
            P("sp", "tp", None),
        ),
        out_specs=(
            P("sp", "tp"),
            P("sp", "tp"),
            P("sp", "tp"),
            P("sp", "tp"),
            P("sp", "tp"),
            P("sp", None, "tp"),
            P("sp", None, "tp"),
            P("sp", "tp", None),
        ),
        check_vma=False,
    )
```

```python
import jax
import jax.numpy as jnp
from jax import lax
from jax.experimental import pallas as pl
from jax.experimental.pallas import tpu as pltpu
from jax.sharding import PartitionSpec as P

EPSILON = 1e-06


def contract_rows(left, right):
    return lax.dot_general(
        left, right, (((0,), (0,)), ((), ())), preferred_element_type=jnp.float32
    )


def contract_cols(left, right):
    return lax.dot_general(
        left, right, (((1,), (1,)), ((), ())), preferred_element_type=jnp.float32
    )


MESH = pl.DeviceIdType.MESH
MIB = 2**20


def layer_kernel(
    planes,
    group,
    stream_hbm,
    gain_hbm,
    cot_hbm,
    weight_hbm,
    route_hbm,
    u_hbm,
    b_hbm,
    c_hbm,
    taps_hbm,
    proj_hbm,
    gate_hbm,
    up_hbm,
    down_hbm,
    grad_ref,
    proj_out,
    u_out,
    b_out,
    c_out,
    *rest,
):
    pieces = rest[:12]
    (
        gain_ref,
        weight_ref,
        route_ref,
        taps_ref,
        column,
        outgoing,
        rows_ref,
        gate_w,
        up_w,
        down_w,
        hidden_ref,
        gate_pre_ref,
        up_pre_ref,
        part_ref,
        theirs_ref,
        ret_ref,
            u_ref,
        b_ref,
        c_ref,
            near_ref,
        rim_ref,
        small_ref,
        square_ref,
        square_other,
        inner_ref,
        inner_other,
        select_ref,
            spots_ref,
        total_ref,
        grad_other,
        block_ref,
            stack_ref,
        edge_ref,
        edge_next,
        turn_ref,
        load,
        hop_send,
        hop_recv,
        plane_send,
        plane_recv,
        cross_send,
        cross_recv,
        part_send,
        part_recv,
        back_send,
        back_recv,
        small_send,
        small_recv,
        rim_send,
        rim_recv,
        side_send,
        side_recv,
        mixed_send,
        mixed_recv,
        spread_send,
        spread_recv,
        pass_send,
        pass_recv,
        share_send,
        share_recv,
        edge_send,
        edge_recv,
    ) = rest[12:]
    count = planes * group
    me = lax.axis_index("sp")
    side = lax.axis_index("tp")
    other = 1 - side
    here = lax.div(me, group)
    place = lax.rem(me, group)
    tokens = grad_ref.shape[0]
    width = column.shape[3]
    bunch = outgoing.shape[2]
    capacity = bunch // group
    f32, bf16 = jnp.float32, jnp.bfloat16

    def local(i, source, target):
        return pltpu.make_async_copy(source, target, load.at[i])

    def remote(source, target, sent, received, **peer):
        return pltpu.make_async_remote_copy(
            src_ref=source,
            dst_ref=target,
            send_sem=sent,
            recv_sem=received,
            device_id=peer,
            device_id_type=MESH,
        )

    loads = [
        local(0, cot_hbm.at[0, :, 0:width], column.at[here, 0]),
        local(1, cot_hbm.at[0, :, width : 2 * width], column.at[here, 1]),
        local(2, stream_hbm.at[0], grad_ref),
        local(3, u_hbm.at[0], u_ref),
        local(4, c_hbm.at[0], c_ref),
        local(5, b_hbm.at[0], b_ref),
        local(6, gate_hbm.at[0], gate_w),
        local(7, up_hbm.at[0], up_w),
        local(8, down_hbm.at[0], down_w),
        local(9, proj_hbm.at[0], gate_w),
        local(10, route_hbm, route_ref),
        local(11, weight_hbm, weight_ref),
        local(12, gain_hbm, gain_ref),
        local(13, taps_hbm, taps_ref),
    ]
    for copy in loads[10:] + loads[:9]:
        copy.start()

    def hop(way, block, piece):
        spot = column.at[block, piece]
        return remote(
            spot,
            spot,
            hop_send.at[way, block],
            hop_recv.at[block, piece],
            sp=me + (1 - 2 * way) * group,
        )

    def onward(way, block, piece):
        room = here < planes - 1 if way == 0 else here > 0

        @pl.when(room)
        def _():
            hop(way, block, piece).start()

    def small(i):
        return remote(
            small_ref.at[here],
            small_ref.at[here],
            small_send,
            small_recv,
            sp=lax.rem(here + i, planes) * group + place,
        )

    def every(spot, sent, received):
        return remote(spot, spot, sent, received, tp=other)

    def stripe(piece):
        return lax.div(piece, 2), 2 * side + lax.rem(piece, 2)

    def span(start, size):
        return pl.ds(pl.multiple_of(start, size), size)

    def inplane(block, piece, i):
        target = lax.rem(place + i, group)
        kind, part = stripe(piece)
        return remote(
            outgoing.at[block, piece, span(target * capacity, capacity)],
            rows_ref.at[kind, part, span(block * bunch + place * capacity, capacity)],
            plane_send.at[block],
            plane_recv.at[block, piece],
            sp=here * group + target,
        )

    def cross(block, piece):
        kind, part = stripe(piece)
        spot = rows_ref.at[kind, part, span(block * bunch, bunch)]
        return remote(
            spot, spot, cross_send.at[block], cross_recv.at[block, piece], tp=other
        )

    def part_copy(block, half):
        return remote(
            part_ref.at[:, half * width : (half + 1) * width],
            theirs_ref.at[block, :, half * width : (half + 1) * width],
            part_send.at[half],
            part_recv.at[block, half],
            tp=other,
        )

    def back(block, i):
        return remote(
            theirs_ref.at[block, span(i * capacity, capacity)],
            ret_ref.at[span(me * capacity, capacity)],
            back_send.at[block],
            back_recv.at[here],
            sp=block * group + i,
        )

    def backs(block, rows):
        return every(
            ret_ref.at[pl.ds(0, rows * capacity)], back_send.at[block], back_recv.at[block]
        )

    def for_backs(block, act):
        @pl.when(block == here)
        def _():
            act(backs(block, group - 1))

        @pl.when(block != here)
        def _():
            act(backs(block, group))

    rim = rim_ref.shape[1]

    def rim_copy(i):
        source = (u_ref, c_ref)[i]
        return remote(
            source.at[tokens - rim : tokens],
            rim_ref.at[i],
            rim_send,
            rim_recv,
            sp=me + 1,
        )

    rims = every(rim_ref, rim_send, rim_recv)
    mixes = every(near_ref.at[pl.ds(0, (group - 1) * tokens)], mixed_send, mixed_recv)

    def mixed(i):
        return remote(
            near_ref.at[span(place * tokens, tokens)],
            near_ref.at[span(place * tokens, tokens)],
            mixed_send,
            mixed_recv,
            sp=here * group + lax.rem(place + i, group),
        )

    def swap(i):
        mine, yours = (
            (square_ref, square_other),
            (inner_ref, inner_other),
            (grad_ref, grad_other),
        )[i]
        return remote(mine, yours, side_send.at[i], side_recv.at[i], tp=other)

    parts, sliver = block_ref.shape[0], block_ref.shape[2]
    per_part = planes // parts
    near = parts // 2
    depth = proj_out.shape[0]
    plain = per_part == 1

    def owned(part):
        return lax.div(part, near) == side

    def strip(target, part):
        if plain:
            start = ((part - side * near) * group + target) * sliver
        else:
            start = (target * near + part - side * near) * sliver
        return (grad_ref if plain else turn_ref).at[:, span(start, sliver)]

    def spread(target, part):
        return remote(
            strip(target, part),
            block_ref.at[part, span(place * tokens, tokens)],
            spread_send.at[part],
            spread_recv.at[part],
            sp=here * group + target,
        )

    def spreads(part):
        spot = block_ref.at[part, pl.ds(0, (group - 1) * tokens)]
        return every(spot, spread_send.at[part], spread_recv.at[part])

    def hand(part):
        spot = block_ref.at[part]
        return remote(spot, spot, pass_send.at[part], pass_recv.at[part], tp=other)

    def share(part, j):
        target = part * per_part + j
        return remote(
            gate_pre_ref.at[span(part * sliver + j * depth, depth)],
            stack_ref.at[here],
            share_send,
            share_recv.at[here],
            sp=target * group + place,
        )

    def share_from(source):
        return remote(
            gate_pre_ref.at[pl.ds(0, depth)],
            stack_ref.at[source],
            share_send,
            share_recv.at[source],
            sp=source * group + place,
        )

    edge_copy = remote(edge_ref, edge_next, edge_send, edge_recv, sp=me - 1)


    def places(block):
        wanted = lax.broadcasted_iota(jnp.int32, (bunch, tokens), 0) + here * bunch
        wanted = wanted.astype(f32)
        return wanted == small_ref[block, 0:1, :], wanted == small_ref[block, 1:2, :]

    def prepare(block, way):
        first, second = places(block)
        select_ref[way] = jnp.where(first | second, 1.0, 0.0).astype(bf16)

    def pick(block, way, piece):
        chosen = jnp.dot(select_ref[way], column[block, piece], preferred_element_type=f32)

        first, second = places(block)
        weight = jnp.where(first, small_ref[block, 2:3, :], 0.0)
        weight += jnp.where(second, small_ref[block, 3:4, :], 0.0)
        scale = jnp.where(piece < 2, jnp.sum(weight, axis=1, keepdims=True), 1.0)
        outgoing[block, piece] = (chosen * scale).astype(bf16)
        kind, part = stripe(piece)
        rows_ref[kind, part, span(block * bunch + place * capacity, capacity)] = outgoing[
            block, piece, span(place * capacity, capacity)
        ]

        @pl.loop(1, group)
        def _(i):
            inplane(block, piece, i).start()

    barrier = pltpu.get_barrier_semaphore()

    @pl.loop(1, count)
    def _(i):
        pl.semaphore_signal(
            barrier, inc=1, device_id={"sp": lax.rem(me + i, count)}, device_id_type=MESH
        )

    pl.semaphore_signal(barrier, inc=1, device_id={"tp": other}, device_id_type=MESH)
    with jax.named_scope("slots"):
        for i in range(10, 14):
            loads[i].wait()
        names = route_ref[...].astype(f32)
        expert_row = lax.broadcasted_iota(jnp.int32, (count, tokens), 0).astype(f32)
        named = [jnp.where(expert_row == names[k : k + 1, :], 1.0, 0.0) for k in range(2)]
        earlier = lax.broadcasted_iota(jnp.int32, (tokens, tokens), 0) < lax.broadcasted_iota(
            jnp.int32, (tokens, tokens), 1
        )
        before = jnp.dot(
            (named[0] + named[1]).astype(bf16),
            jnp.where(earlier, 1.0, 0.0).astype(bf16),
            preferred_element_type=f32,
        )
        slots = [
            names[k : k + 1, :] * capacity + jnp.sum(named[k] * before, axis=0, keepdims=True)
            for k in range(2)
        ]
        info = jnp.concatenate(
            slots + [weight_ref[...], jnp.zeros((4, tokens), f32)], axis=0
        )
        small_ref[here] = info
        lanes = square_ref.shape[1]
        loads[2].wait()
        total = jnp.zeros((tokens, lanes), f32)
        for start in range(0, 2 * width, lanes):
            value = grad_ref[:, start : start + lanes].astype(f32)
            total = total + value * value
        square_ref[...] = total
        loads[0].wait()
        loads[1].wait()
    with jax.named_scope("greet"):
        pl.semaphore_wait(barrier, count)
    with jax.named_scope("own"):
        swap(0).start()

        @pl.loop(1, planes)
        def _(i):
            small(i).start()

        for i in range(3, 5):
            loads[i].wait()

        @pl.when(me < count - 1)
        def _():
            for i in range(2):
                rim_copy(i).start()

        for piece in range(2):
            for way in range(2):
                onward(way, here, piece)
        prepare(here, 0)
        for piece in range(2):
            pick(here, 0, jnp.int32(piece))
        swap(0).wait_recv()
        total = square_ref[...] + square_other[...]
        inverse = lax.rsqrt(jnp.sum(total, axis=1, keepdims=True) / (4 * width) + EPSILON)
        for piece in range(2):
            cols = slice(piece * width, (piece + 1) * width)
            value = grad_ref[:, cols].astype(f32) * inverse * gain_ref[:, cols]
            column[here, 2 + piece] = value.astype(bf16)
        for piece in range(2, 4):
            for way in range(2):
                onward(way, here, piece)
        for piece in range(2, 4):
            pick(here, 0, jnp.int32(piece))
        @pl.when(me == 0)
        def _():
            rim_ref[...] = jnp.zeros_like(rim_ref)

        spots_ref[...] = jnp.transpose(small_ref[here])

        smalls = every(small_ref.at[pl.ds(0, planes - 1)], small_send, small_recv)
        smalls.wait_recv()

        for i in range(5, 9):
            loads[i].wait()

    def arrive(step, piece):
        for way in range(2):
            block = here - step if way == 0 else here + step
            valid = (step < planes) & (block >= 0) & (block < planes)

            @pl.when(valid)
            def _():
                hop(way, block, piece).wait_recv()
                onward(way, block, piece)

        for way in range(2):
            block = here - step if way == 0 else here + step
            valid = (step < planes) & (block >= 0) & (block < planes)

            @pl.when(valid)
            def _():
                @pl.when(piece == 0)
                def _():
                    prepare(block, way)

                pick(block, way, piece)

    def collect(block, piece):
        spot = outgoing.at[block, piece, pl.ds(0, (group - 1) * capacity)]
        every(spot, plane_send.at[block], plane_recv.at[block, piece]).wait_recv()
        cross(block, piece).start()

    def gather(step, way):
        block = here - step + 2 * way * step
        valid = (block >= 0) & (block < planes) & ((way == 0) | (step > 0))

        @pl.when(valid)
        def _():
            @pl.loop(0, 3)
            def _(piece):
                collect(block, piece)

    def compute(step, way):
        block = here - step + 2 * way * step
        valid = (block >= 0) & (block < planes) & ((way == 0) | (step > 0))

        @pl.when(valid)
        def _():
            rows = span(block * bunch, bunch)
            gate_lin = jnp.zeros((bunch, gate_w.shape[1]), f32)
            up_lin = jnp.zeros((bunch, gate_w.shape[1]), f32)
            hidden_grad = jnp.zeros((bunch, gate_w.shape[1]), f32)
            for piece in range(2):
                cross(block, piece).wait_recv()
            for part in range(4):
                cols = slice(part * width, (part + 1) * width)
                hidden_grad += contract_cols(rows_ref[0, part, rows], down_w[:, cols])
            for piece in range(2, 4):
                if piece == 3:
                    collect(block, piece)
                cross(block, piece).wait_recv()
                for part in range(piece - 2, 4, 2):
                    cols = slice(part * width, (part + 1) * width)
                    inputs = rows_ref[1, part, rows]
                    gate_lin += jnp.dot(inputs, gate_w[cols], preferred_element_type=f32)
                    up_lin += jnp.dot(inputs, up_w[cols], preferred_element_type=f32)
            sigmoid_gate = jax.nn.sigmoid(gate_lin)
            silu_gate = gate_lin * sigmoid_gate
            hidden_ref[rows] = (silu_gate * up_lin).astype(bf16)
            gate_pre = (
                hidden_grad * up_lin * sigmoid_gate * (1.0 + gate_lin * (1.0 - sigmoid_gate))
            ).astype(bf16)
            up_pre = (hidden_grad * silu_gate).astype(bf16)
            gate_pre_ref[rows] = gate_pre
            up_pre_ref[rows] = up_pre

            def partial(whose, half):
                spot = span((2 * whose + half) * width, width)
                value = contract_cols(gate_pre_ref[rows], gate_w[spot])
                value += contract_cols(up_pre_ref[rows], up_w[spot])
                return value.astype(bf16)

            for half in range(2):
                part_ref[:, half * width : (half + 1) * width] = partial(other, half)
                part_copy(block, half).start()
            for half in range(2):
                cols = slice(half * width, (half + 1) * width)
                mine = partial(side, half).astype(f32)
                part_copy(block, half).wait_recv()
                theirs = theirs_ref[block, :, cols].astype(f32)
                theirs_ref[block, :, cols] = (mine + theirs).astype(bf16)
            for half in range(2):
                part_copy(block, half).wait_send()

    def reply(step, way):
        block = here - step + 2 * way * step
        valid = (block >= 0) & (block < planes) & ((way == 0) | (step > 0))

        @pl.when(valid)
        def _():
            @pl.loop(0, group)
            def _(turn):
                i = lax.rem(place + turn, group)

                @pl.when(block * group + i != me)
                def _():
                    back(block, i).start()

                @pl.when(block * group + i == me)
                def _():
                    ret_ref[span(me * capacity, capacity)] = theirs_ref[
                        block, span(i * capacity, capacity)
                    ]

    def convolve():
        gated = c_ref[...].astype(f32) * u_ref[...].astype(f32)
        rim_gated = rim_ref[1].astype(f32) * rim_ref[0].astype(f32)
        row = lax.broadcasted_iota(jnp.int32, gated.shape, 0)
        one = jnp.where(row == 0, rim_gated[rim - 1 : rim], pltpu.roll(gated, 1, 0))
        two = jnp.where(
            row == 0,
            rim_gated[rim - 2 : rim - 1],
            jnp.where(row == 1, rim_gated[rim - 1 : rim], pltpu.roll(gated, 2, 0)),
        )
        conv = taps_ref[0:1, :] * two + taps_ref[1:2, :] * one + taps_ref[2:3, :] * gated
        return conv

    inside = (here > 0) & (here < planes - 1)

    @pl.loop(1, planes + 1)
    def _(step):
        with jax.named_scope("arrive0"):

            @pl.loop(0, 2)
            def _(piece):
                arrive(step, piece)

        with jax.named_scope("gather"):

            @pl.loop(0, 2)
            def _(way):
                gather(step - 1, way)

        @pl.loop(0, 2)
        def _(way):
            with jax.named_scope("compute"):
                compute(step - 1, way)

        with jax.named_scope("arrive2"):

            @pl.loop(2, 4)
            def _(piece):
                arrive(step, piece)

        @pl.loop(0, 2)
        def _(way):
            reply(step - 1, way)

        @pl.when(step == 1)
        def _():
            @pl.when(me > 0)
            def _():
                rims.wait_recv()

            mixed_value = b_ref[...].astype(f32) * convolve()
            near_ref[span(place * tokens, tokens)] = mixed_value.astype(bf16)

        @pl.when(step == jnp.where(inside, planes, 2))
        def _():
            @pl.loop(1, group)
            def _(i):
                mixed(i).start()

    loads[9].start()
    with jax.named_scope("wgrad"):

        for part in range(4):
            inputs = rows_ref[1, part]
            pieces[part][...] = contract_rows(inputs, gate_pre_ref[...])
            pieces[4 + part][...] = contract_rows(inputs, up_pre_ref[...])
            pieces[8 + part][...] = contract_rows(hidden_ref[...], rows_ref[0, part])

    @pl.loop(0, planes)
    def _(block):
        for way in range(2):
            room = here < planes - 1 if way == 0 else here > 0
            mine = block <= here if way == 0 else block >= here

            @pl.when(room & mine)
            def _():
                every(column.at[block], hop_send.at[way, block], hop_recv.at[0, 0]).wait_send()

        every(outgoing.at[block], cross_send.at[block], cross_recv.at[0, 0]).wait_send()
        spot = outgoing.at[block, :, pl.ds(0, (group - 1) * capacity)]
        every(spot, plane_send.at[block], plane_recv.at[0, 0]).wait_send()

    smalls.wait_send()

    @pl.when(me < count - 1)
    def _():
        rims.wait_send()

    swap(0).wait_send()

    @pl.loop(0, planes)
    def _(turn):
        block = lax.rem(here + turn, planes)
        with jax.named_scope("returned"):

            for_backs(block, lambda copy: copy.wait_recv())

        with jax.named_scope("pull"):
            rows = span(block * bunch, bunch)
            slot = lax.broadcasted_iota(jnp.int32, (tokens, bunch), 1) + block * bunch
            slot = slot.astype(f32)
            hit = (slot == spots_ref[:, 0:1]) | (slot == spots_ref[:, 1:2])
            pull = jnp.where(hit, 1.0, 0.0).astype(bf16)
            value = jnp.dot(pull, ret_ref[rows], preferred_element_type=f32)

            @pl.when(turn == 0)
            def _():
                total_ref[...] = value

            @pl.when(turn > 0)
            def _():
                total_ref[...] += value

    with jax.named_scope("cross"):
        total = jnp.zeros((tokens, lanes), f32)
        for start in range(0, 2 * width, lanes):
            cols = slice(start, start + lanes)
            total += grad_ref[:, cols].astype(f32) * gain_ref[:, cols] * total_ref[:, cols]
        inner_ref[...] = total
        swap(1).start()
        square = jnp.sum(square_ref[...] + square_other[...], axis=1, keepdims=True)
        inverse = lax.rsqrt(square / (4 * width) + EPSILON)
        swap(1).wait_recv()
        inner = jnp.sum(inner_ref[...] + inner_other[...], axis=1, keepdims=True)
        pull_back = inverse * inverse * inverse * inner / (4 * width)
        for piece in range(2):
            cols = slice(piece * width, (piece + 1) * width)
            grad_ref[:, cols] = (
                column[here, piece].astype(f32)
                + inverse * gain_ref[:, cols] * total_ref[:, cols]
                - grad_ref[:, cols].astype(f32) * pull_back
            ).astype(bf16)
        swap(2).start()

    upper = here >= planes // 2
    base = lax.div(here * parts, planes)

    def turned(k):
        return lax.rem(base + parts + jnp.where(upper, 1 + k, parts - 1 - k), parts)

    with jax.named_scope("spread"):

        if not plain:
            features = 2 * width
            run = near * sliver
            for start in range(0, features, sliver):
                goal = lax.broadcasted_iota(jnp.int32, (features, sliver), 1) + start
                inner_goal = lax.rem(goal, run)
                origin = (
                    lax.div(inner_goal, depth) * group + lax.div(goal, run)
                ) * depth + lax.rem(inner_goal, depth)
                match = lax.broadcasted_iota(jnp.int32, (features, sliver), 0) == origin
                turn_ref[:, start : start + sliver] = jnp.dot(
                    grad_ref[...],
                    jnp.where(match, 1.0, 0.0).astype(bf16),
                    preferred_element_type=f32,
                ).astype(bf16)

        def spread_all():
            @pl.loop(0, parts)
            def _(k):
                part = turned(k)

                @pl.when(owned(part))
                def _():
                    @pl.loop(0, group)
                    def _(target):
                        @pl.when(target != place)
                        def _():
                            spread(target, part).start()

                    block_ref[part, span(place * tokens, tokens)] = strip(place, part)[...]

        first = owned(turned(0))

        @pl.when(first)
        def _():
            spread_all()

    with jax.named_scope("mixer"):
        half = 2 * width
        loads[9].wait()
        mixer_grad = jnp.dot(
            grad_ref[...], gate_w[span(side * half, half)], preferred_element_type=f32
        )
        swap(2).wait_recv()
        mixer_grad += jnp.dot(
            grad_other[...], gate_w[span(other * half, half)], preferred_element_type=f32
        )
        delta = mixer_grad * b_ref[...].astype(f32)
        edge_ref[...] = delta[0 : edge_ref.shape[0]]

        @pl.when(me > 0)
        def _():
            edge_copy.start()

        b_out[...] = (mixer_grad * convolve()).astype(bf16)

    @pl.when(jnp.logical_not(first))
    def _():
        spread_all()

    mixes.wait()

    @pl.loop(0, parts)
    def _(k):
        part = turned(k)
        with jax.named_scope("collect"):

            @pl.when(owned(part))
            def _():
                spreads(part).wait_recv()
                hand(part).start()

            @pl.when(jnp.logical_not(owned(part)))
            def _():
                hand(part).wait_recv()

        with jax.named_scope("shares"):
            value = contract_rows(block_ref[part], near_ref[...])
            gate_pre_ref[span(part * sliver, sliver)] = value.astype(bf16)
            for j in range(per_part):

                @pl.when(part * per_part + j != here)
                def _():
                    share(part, j).start()

                @pl.when(part * per_part + j == here)
                def _():
                    proj_out[...] = value[j * depth : (j + 1) * depth]

    with jax.named_scope("edge"):

        @pl.when(me == count - 1)
        def _():
            edge_next[...] = jnp.zeros_like(edge_next)

        @pl.when(me < count - 1)
        def _():
            edge_copy.wait_recv()

        row = lax.broadcasted_iota(jnp.int32, delta.shape, 0)
        one = jnp.where(
            row == tokens - 1, edge_next[0:1], pltpu.roll(delta, tokens - 1, 0)
        )
        two = jnp.where(
            row == tokens - 2,
            edge_next[0:1],
            jnp.where(row == tokens - 1, edge_next[1:2], pltpu.roll(delta, tokens - 2, 0)),
        )
        gated_grad = taps_ref[2:3, :] * delta + taps_ref[1:2, :] * one + taps_ref[0:1, :] * two
        u_out[...] = (gated_grad * c_ref[...].astype(f32)).astype(bf16)
        c_out[...] = (gated_grad * u_ref[...].astype(f32)).astype(bf16)

    @pl.loop(0, planes)
    def _(block):
        for_backs(block, lambda copy: copy.wait_send())

    @pl.when(me > 0)
    def _():
        edge_copy.wait_send()

    for i in range(1, 3):
        swap(i).wait_send()

    @pl.loop(0, parts)
    def _(part):
        @pl.when(owned(part))
        def _():
            spreads(part).wait_send()
            hand(part).wait_send()

    with jax.named_scope("final"):

        @pl.loop(1, planes)
        def _(i):
            source = lax.rem(here + i, planes)
            share_from(source).wait_recv()
            proj_out[...] += stack_ref[source].astype(f32)

    every(stack_ref.at[pl.ds(0, planes - 1)], share_send, share_recv.at[0]).wait_send()


def store_kernel(*refs):
    sources, targets, sems = refs[:17], refs[17:25], refs[25]
    copies = []
    for i in range(17):
        if i < 5:
            target = targets[i]
        else:
            which, part = (i - 5) // 4, (i - 5) % 4
            rows, cols = sources[i].shape
            target = targets[5 + which]
            if which < 2:
                target = target.at[pl.ds(part * rows, rows)]
            else:
                target = target.at[:, pl.ds(part * cols, cols)]
        copies.append(pltpu.make_async_copy(sources[i], target, sems.at[i]))
    for copy in copies:
        copy.start()
    for copy in copies:
        copy.wait()


def pinned(value):
    return pltpu.with_memory_space_constraint(value, pltpu.HBM)


def local(
    stream,
    norm_gain,
    cotangent,
    route_weights,
    routes,
    conv_input,
    conv_bgate,
    conv_cgate,
    conv_taps,
    out_proj,
    gate_weight,
    up_weight,
    down_weight,
):
    count = lax.axis_size("sp")
    group = 2 ** ((count.bit_length() - 1) // 2)
    planes = count // group
    tokens, features = stream.shape
    width = features // 2
    channels = conv_input.shape[1]
    gate_shape, down_shape = gate_weight.shape[1:], down_weight.shape[1:]
    hidden = gate_shape[1]
    capacity = 2 * tokens * routes.shape[1] // count
    bunch = group * capacity
    slots = count * capacity
    grant = 38 * MIB + 2 * planes * tokens * features * 2
    depth = 2 * features // count
    sliver = max(128, depth)
    parts = planes * depth // sliver
    f32, bf16 = jnp.float32, jnp.bfloat16
    shape = jax.ShapeDtypeStruct
    outs = (
        shape(stream.shape, bf16),
        shape((depth, channels), f32),
        shape(conv_input.shape, bf16),
        shape(conv_input.shape, bf16),
        shape(conv_input.shape, bf16),
        shape(gate_shape, f32),
        shape(gate_shape, f32),
        shape(down_shape, f32),
    )
    vmem, hbm = pl.BlockSpec(memory_space=pltpu.VMEM), pl.BlockSpec(memory_space=pltpu.HBM)
    dma = pltpu.SemaphoreType.DMA
    results = pl.pallas_call(
        lambda *refs: layer_kernel(planes, group, *refs),
        out_shape=tuple(pltpu.VMEM(out.shape, out.dtype) for out in outs[:5])
        + (pltpu.VMEM((width, hidden), f32),) * 8
        + (pltpu.VMEM((hidden, width), f32),) * 4,
        in_specs=[hbm] * 13,
        out_specs=[vmem] * 17,
        scratch_shapes=[
            pltpu.VMEM((1, features), f32),
            pltpu.VMEM(route_weights.shape[::-1], f32),
            pltpu.VMEM(routes.shape[::-1], jnp.int32),
            pltpu.VMEM(conv_taps.shape, f32),
            pltpu.VMEM((planes, 4, tokens, width), bf16),
            pltpu.VMEM((planes, 4, bunch, width), bf16),
            pltpu.VMEM((2, 4, slots, width), bf16),
            pltpu.VMEM(gate_shape, bf16),
            pltpu.VMEM(gate_shape, bf16),
            pltpu.VMEM(down_shape, bf16),
            pltpu.VMEM((slots, hidden), bf16),
            pltpu.VMEM((slots, hidden), bf16),
            pltpu.VMEM((slots, hidden), bf16),
            pltpu.VMEM((bunch, features), bf16),
            pltpu.VMEM((planes, bunch, features), bf16),
            pltpu.VMEM((slots, features), bf16),
            pltpu.VMEM((tokens, channels), bf16),
            pltpu.VMEM((tokens, channels), bf16),
            pltpu.VMEM((tokens, channels), bf16),
            pltpu.VMEM((group * tokens, channels), bf16),
            pltpu.VMEM((2, 16, channels), bf16),
            pltpu.VMEM((planes, 8, tokens), f32),
            pltpu.VMEM((tokens, 128), f32),
            pltpu.VMEM((tokens, 128), f32),
            pltpu.VMEM((tokens, 128), f32),
            pltpu.VMEM((tokens, 128), f32),
            pltpu.VMEM((2, bunch, tokens), bf16),
            pltpu.VMEM((tokens, 8), f32),
            pltpu.VMEM((tokens, features), f32),
            pltpu.VMEM((tokens, features), bf16),
            pltpu.VMEM((parts, group * tokens, sliver), bf16),
            pltpu.VMEM((planes, depth, channels), bf16),
            pltpu.VMEM((8, channels), f32),
            pltpu.VMEM((8, channels), f32),
            pltpu.VMEM(stream.shape if sliver > depth else (8, 128), bf16),
            dma((14,)),
            dma((2, planes)),
            dma((planes, 4)),
            dma((planes,)),
            dma((planes, 4)),
            dma((planes,)),
            dma((planes, 4)),
            dma((2,)),
            dma((planes, 2)),
            dma((planes,)),
            dma((planes,)),
            dma,
            dma,
            dma,
            dma,
            dma((3,)),
            dma((3,)),
            dma,
            dma,
            dma((parts,)),
            dma((parts,)),
            dma((parts,)),
            dma((parts,)),
            dma,
            dma((planes,)),
            dma,
            dma,
        ],
        compiler_params=pltpu.CompilerParams(
            collective_id=0, has_side_effects=True, vmem_limit_bytes=grant
        ),
        name="layer",
    )(
        pinned(stream[None]),
        pinned(norm_gain[None, :]),
        pinned(cotangent[None]),
        pinned(route_weights.T),
        pinned(routes.T),
        pinned(conv_input[None]),
        pinned(conv_bgate[None]),
        pinned(conv_cgate[None]),
        pinned(conv_taps),
        pinned(out_proj[None]),
        pinned(gate_weight),
        pinned(up_weight),
        pinned(down_weight),
    )
    results = pl.pallas_call(
        store_kernel,
        out_shape=outs,
        in_specs=[vmem] * 17,
        out_specs=[hbm] * 8,
        scratch_shapes=[dma((17,))],
        compiler_params=pltpu.CompilerParams(vmem_limit_bytes=2**20),
        name="store",
    )(*results)
    return tuple(results[:5]) + tuple(value[None] for value in results[5:])


def solution(mesh):
    return jax.shard_map(
        local,
        mesh=mesh,
        in_specs=(
            P("sp", "tp"),
            P("tp"),
            P("sp", "tp"),
            P("sp", None),
            P("sp", None),
            P("sp", "tp"),
            P("sp", "tp"),
            P("sp", "tp"),
            P(None, "tp"),
            P(None, "tp"),
            P("sp", None, "tp"),
            P("sp", None, "tp"),
            P("sp", "tp", None),
        ),
        out_specs=(
            P("sp", "tp"),
            P("sp", "tp"),
            P("sp", "tp"),
            P("sp", "tp"),
            P("sp", "tp"),
            P("sp", None, "tp"),
            P("sp", None, "tp"),
            P("sp", "tp", None),
        ),
        check_vma=False,
    )
```

```python
import jax
import jax.numpy as jnp
from jax import lax
from jax.experimental import pallas as pl
from jax.experimental.pallas import tpu as pltpu
from jax.sharding import PartitionSpec as P

EPSILON = 1e-06


def contract_rows(left, right):
    return lax.dot_general(
        left, right, (((0,), (0,)), ((), ())), preferred_element_type=jnp.float32
    )


def contract_cols(left, right):
    return lax.dot_general(
        left, right, (((1,), (1,)), ((), ())), preferred_element_type=jnp.float32
    )


MESH = pl.DeviceIdType.MESH
MIB = 2**20


def layer_kernel(
    planes,
    group,
    stream_hbm,
    gain_hbm,
    cot_hbm,
    weight_hbm,
    route_hbm,
    u_hbm,
    b_hbm,
    c_hbm,
    taps_hbm,
    proj_hbm,
    gate_hbm,
    up_hbm,
    down_hbm,
    grad_ref,
    proj_out,
    u_out,
    b_out,
    c_out,
    *rest,
):
    pieces = rest[:12]
    (
        gain_ref,
        weight_ref,
        route_ref,
        taps_ref,
        column,
        outgoing,
        rows_ref,
        gate_w,
        up_w,
        down_w,
        hidden_ref,
        gate_pre_ref,
        up_pre_ref,
        part_ref,
        theirs_ref,
        ret_ref,
            u_ref,
        b_ref,
        c_ref,
            near_ref,
        rim_ref,
        small_ref,
        square_ref,
        square_other,
        inner_ref,
        inner_other,
        select_ref,
            spots_ref,
        total_ref,
        grad_other,
        block_ref,
            stack_ref,
        edge_ref,
        edge_next,
        turn_ref,
        load,
        hop_send,
        hop_recv,
        plane_send,
        plane_recv,
        cross_send,
        cross_recv,
        part_send,
        part_recv,
        back_send,
        back_recv,
        small_send,
        small_recv,
        rim_send,
        rim_recv,
        side_send,
        side_recv,
        mixed_send,
        mixed_recv,
        spread_send,
        spread_recv,
        pass_send,
        pass_recv,
        share_send,
        share_recv,
        edge_send,
        edge_recv,
    ) = rest[12:]
    count = planes * group
    me = lax.axis_index("sp")
    side = lax.axis_index("tp")
    other = 1 - side
    here = lax.div(me, group)
    place = lax.rem(me, group)
    tokens = grad_ref.shape[0]
    width = column.shape[3]
    bunch = outgoing.shape[2]
    capacity = bunch // group
    f32, bf16 = jnp.float32, jnp.bfloat16

    def local(i, source, target):
        return pltpu.make_async_copy(source, target, load.at[i])

    def remote(source, target, sent, received, **peer):
        return pltpu.make_async_remote_copy(
            src_ref=source,
            dst_ref=target,
            send_sem=sent,
            recv_sem=received,
            device_id=peer,
            device_id_type=MESH,
        )

    loads = [
        local(0, cot_hbm.at[0, :, 0:width], column.at[here, 0]),
        local(1, cot_hbm.at[0, :, width : 2 * width], column.at[here, 1]),
        local(2, stream_hbm.at[0], grad_ref),
        local(3, u_hbm.at[0], u_ref),
        local(4, c_hbm.at[0], c_ref),
        local(5, b_hbm.at[0], b_ref),
        local(6, gate_hbm.at[0], gate_w),
        local(7, up_hbm.at[0], up_w),
        local(8, down_hbm.at[0], down_w),
        local(9, proj_hbm.at[0], gate_w),
        local(10, route_hbm, route_ref),
        local(11, weight_hbm, weight_ref),
        local(12, gain_hbm, gain_ref),
        local(13, taps_hbm, taps_ref),
    ]
    for copy in loads[10:] + loads[:9]:
        copy.start()

    def hop(way, block, piece):
        spot = column.at[block, piece]
        return remote(
            spot,
            spot,
            hop_send.at[way, block],
            hop_recv.at[block, piece],
            sp=me + (1 - 2 * way) * group,
        )

    def onward(way, block, piece):
        room = here < planes - 1 if way == 0 else here > 0

        @pl.when(room)
        def _():
            hop(way, block, piece).start()

    def small(i):
        return remote(
            small_ref.at[here],
            small_ref.at[here],
            small_send,
            small_recv,
            sp=lax.rem(here + i, planes) * group + place,
        )

    def every(spot, sent, received):
        return remote(spot, spot, sent, received, tp=other)

    def stripe(piece):
        return lax.div(piece, 2), 2 * side + lax.rem(piece, 2)

    def span(start, size):
        return pl.ds(pl.multiple_of(start, size), size)

    def inplane(block, piece, i):
        target = lax.rem(place + i, group)
        kind, part = stripe(piece)
        return remote(
            outgoing.at[block, piece, span(target * capacity, capacity)],
            rows_ref.at[kind, part, span(block * bunch + place * capacity, capacity)],
            plane_send,
            plane_recv.at[block, piece],
            sp=here * group + target,
        )

    def cross(block, piece):
        kind, part = stripe(piece)
        spot = rows_ref.at[kind, part, span(block * bunch, bunch)]
        return remote(
            spot, spot, cross_send, cross_recv.at[block, piece], tp=other
        )

    def part_copy(block, half):
        return remote(
            part_ref.at[:, half * width : (half + 1) * width],
            theirs_ref.at[block, :, half * width : (half + 1) * width],
            part_send.at[half],
            part_recv.at[block, half],
            tp=other,
        )

    def back(block, i):
        return remote(
            theirs_ref.at[block, span(i * capacity, capacity)],
            ret_ref.at[span(me * capacity, capacity)],
            back_send,
            back_recv.at[here],
            sp=block * group + i,
        )

    def backs(block, rows):
        return every(
            ret_ref.at[pl.ds(0, rows * capacity)], back_send, back_recv.at[block]
        )

    def for_backs(block, act):
        @pl.when(block == here)
        def _():
            act(backs(block, group - 1))

        @pl.when(block != here)
        def _():
            act(backs(block, group))

    rim = rim_ref.shape[1]

    def rim_copy(i):
        source = (u_ref, c_ref)[i]
        return remote(
            source.at[tokens - rim : tokens],
            rim_ref.at[i],
            rim_send,
            rim_recv,
            sp=me + 1,
        )

    rims = every(rim_ref, rim_send, rim_recv)
    mixes = every(near_ref.at[pl.ds(0, (group - 1) * tokens)], mixed_send, mixed_recv)

    def mixed(i):
        return remote(
            near_ref.at[span(place * tokens, tokens)],
            near_ref.at[span(place * tokens, tokens)],
            mixed_send,
            mixed_recv,
            sp=here * group + lax.rem(place + i, group),
        )

    def swap(i):
        mine, yours = (
            (square_ref, square_other),
            (inner_ref, inner_other),
            (grad_ref, grad_other),
        )[i]
        return remote(mine, yours, side_send.at[i], side_recv.at[i], tp=other)

    parts, sliver = block_ref.shape[0], block_ref.shape[2]
    per_part = planes // parts
    near = parts // 2
    depth = proj_out.shape[0]
    plain = per_part == 1

    def owned(part):
        return lax.div(part, near) == side

    def strip(target, part):
        if plain:
            start = ((part - side * near) * group + target) * sliver
        else:
            start = (target * near + part - side * near) * sliver
        return (grad_ref if plain else turn_ref).at[:, span(start, sliver)]

    def spread(target, part):
        return remote(
            strip(target, part),
            block_ref.at[part, span(place * tokens, tokens)],
            spread_send.at[part],
            spread_recv.at[part],
            sp=here * group + target,
        )

    def spreads(part):
        spot = block_ref.at[part, pl.ds(0, (group - 1) * tokens)]
        return every(spot, spread_send.at[part], spread_recv.at[part])

    def hand(part):
        spot = block_ref.at[part]
        return remote(spot, spot, pass_send.at[part], pass_recv.at[part], tp=other)

    def share(part, j):
        target = part * per_part + j
        return remote(
            gate_pre_ref.at[span(part * sliver + j * depth, depth)],
            stack_ref.at[here],
            share_send,
            share_recv.at[here],
            sp=target * group + place,
        )

    def share_from(source):
        return remote(
            gate_pre_ref.at[pl.ds(0, depth)],
            stack_ref.at[source],
            share_send,
            share_recv.at[source],
            sp=source * group + place,
        )

    edge_copy = remote(edge_ref, edge_next, edge_send, edge_recv, sp=me - 1)


    def places(block):
        wanted = lax.broadcasted_iota(jnp.int32, (bunch, tokens), 0) + here * bunch
        wanted = wanted.astype(f32)
        return wanted == small_ref[block, 0:1, :], wanted == small_ref[block, 1:2, :]

    def prepare(block, way):
        first, second = places(block)
        select_ref[way] = jnp.where(first | second, 1.0, 0.0).astype(bf16)

    def pick(block, way, piece):
        chosen = jnp.dot(select_ref[way], column[block, piece], preferred_element_type=f32)

        first, second = places(block)
        weight = jnp.where(first, small_ref[block, 2:3, :], 0.0)
        weight += jnp.where(second, small_ref[block, 3:4, :], 0.0)
        scale = jnp.where(piece < 2, jnp.sum(weight, axis=1, keepdims=True), 1.0)
        outgoing[block, piece] = (chosen * scale).astype(bf16)
        kind, part = stripe(piece)
        rows_ref[kind, part, span(block * bunch + place * capacity, capacity)] = outgoing[
            block, piece, span(place * capacity, capacity)
        ]

        @pl.loop(1, group)
        def _(i):
            inplane(block, piece, i).start()

    barrier = pltpu.get_barrier_semaphore()

    @pl.loop(1, count)
    def _(i):
        pl.semaphore_signal(
            barrier, inc=1, device_id={"sp": lax.rem(me + i, count)}, device_id_type=MESH
        )

    pl.semaphore_signal(barrier, inc=1, device_id={"tp": other}, device_id_type=MESH)
    with jax.named_scope("slots"):
        for i in range(10, 14):
            loads[i].wait()
        names = route_ref[...].astype(f32)
        expert_row = lax.broadcasted_iota(jnp.int32, (count, tokens), 0).astype(f32)
        named = [jnp.where(expert_row == names[k : k + 1, :], 1.0, 0.0) for k in range(2)]
        earlier = lax.broadcasted_iota(jnp.int32, (tokens, tokens), 0) < lax.broadcasted_iota(
            jnp.int32, (tokens, tokens), 1
        )
        before = jnp.dot(
            (named[0] + named[1]).astype(bf16),
            jnp.where(earlier, 1.0, 0.0).astype(bf16),
            preferred_element_type=f32,
        )
        slots = [
            names[k : k + 1, :] * capacity + jnp.sum(named[k] * before, axis=0, keepdims=True)
            for k in range(2)
        ]
        info = jnp.concatenate(
            slots + [weight_ref[...], jnp.zeros((4, tokens), f32)], axis=0
        )
        small_ref[here] = info
        lanes = square_ref.shape[1]
        loads[2].wait()
        total = jnp.zeros((tokens, lanes), f32)
        for start in range(0, 2 * width, lanes):
            value = grad_ref[:, start : start + lanes].astype(f32)
            total = total + value * value
        square_ref[...] = total
        loads[0].wait()
        loads[1].wait()
    with jax.named_scope("greet"):
        pl.semaphore_wait(barrier, count)
    with jax.named_scope("own"):
        for way in range(2):
            onward(way, here, 0)
        swap(0).start()

        @pl.loop(1, planes)
        def _(i):
            small(i).start()

        for i in range(3, 5):
            loads[i].wait()

        @pl.when(me < count - 1)
        def _():
            for i in range(2):
                rim_copy(i).start()

        for way in range(2):
            onward(way, here, 1)
        prepare(here, 0)
        for piece in range(2):
            pick(here, 0, jnp.int32(piece))
        swap(0).wait_recv()
        total = square_ref[...] + square_other[...]
        inverse = lax.rsqrt(jnp.sum(total, axis=1, keepdims=True) / (4 * width) + EPSILON)
        for piece in range(2):
            cols = slice(piece * width, (piece + 1) * width)
            value = grad_ref[:, cols].astype(f32) * inverse * gain_ref[:, cols]
            column[here, 2 + piece] = value.astype(bf16)
        for piece in range(2, 4):
            for way in range(2):
                onward(way, here, piece)
        for piece in range(2, 4):
            pick(here, 0, jnp.int32(piece))
        @pl.when(me == 0)
        def _():
            rim_ref[...] = jnp.zeros_like(rim_ref)

        spots_ref[...] = jnp.transpose(small_ref[here])

        smalls = every(small_ref.at[pl.ds(0, planes - 1)], small_send, small_recv)
        smalls.wait_recv()

        for i in range(5, 9):
            loads[i].wait()

    def arrive(step, piece):
        for way in range(2):
            block = here - step if way == 0 else here + step
            valid = (step < planes) & (block >= 0) & (block < planes)

            @pl.when(valid)
            def _():
                hop(way, block, piece).wait_recv()
                onward(way, block, piece)

        for way in range(2):
            block = here - step if way == 0 else here + step
            valid = (step < planes) & (block >= 0) & (block < planes)

            @pl.when(valid)
            def _():
                @pl.when(piece == 0)
                def _():
                    prepare(block, way)

                pick(block, way, piece)

    def collect(block, piece):
        spot = outgoing.at[block, piece, pl.ds(0, (group - 1) * capacity)]
        every(spot, plane_send, plane_recv.at[block, piece]).wait_recv()
        cross(block, piece).start()

    def gather(step, way):
        block = here - step + 2 * way * step
        valid = (block >= 0) & (block < planes) & ((way == 0) | (step > 0))

        @pl.when(valid)
        def _():
            @pl.loop(0, 3)
            def _(piece):
                collect(block, piece)

    def compute(step, way):
        block = here - step + 2 * way * step
        valid = (block >= 0) & (block < planes) & ((way == 0) | (step > 0))

        @pl.when(valid)
        def _():
            rows = span(block * bunch, bunch)
            gate_lin = jnp.zeros((bunch, gate_w.shape[1]), f32)
            up_lin = jnp.zeros((bunch, gate_w.shape[1]), f32)
            hidden_grad = jnp.zeros((bunch, gate_w.shape[1]), f32)
            for piece in range(2):
                cross(block, piece).wait_recv()
            for part in range(4):
                cols = slice(part * width, (part + 1) * width)
                hidden_grad += contract_cols(rows_ref[0, part, rows], down_w[:, cols])
            for piece in range(2, 4):
                if piece == 3:
                    collect(block, piece)
                cross(block, piece).wait_recv()
                for part in range(piece - 2, 4, 2):
                    cols = slice(part * width, (part + 1) * width)
                    inputs = rows_ref[1, part, rows]
                    gate_lin += jnp.dot(inputs, gate_w[cols], preferred_element_type=f32)
                    up_lin += jnp.dot(inputs, up_w[cols], preferred_element_type=f32)
            sigmoid_gate = jax.nn.sigmoid(gate_lin)
            silu_gate = gate_lin * sigmoid_gate
            hidden_ref[rows] = (silu_gate * up_lin).astype(bf16)
            gate_pre = (
                hidden_grad * up_lin * sigmoid_gate * (1.0 + gate_lin * (1.0 - sigmoid_gate))
            ).astype(bf16)
            up_pre = (hidden_grad * silu_gate).astype(bf16)
            gate_pre_ref[rows] = gate_pre
            up_pre_ref[rows] = up_pre

            def partial(whose, half):
                spot = span((2 * whose + half) * width, width)
                value = contract_cols(gate_pre_ref[rows], gate_w[spot])
                value += contract_cols(up_pre_ref[rows], up_w[spot])
                return value.astype(bf16)

            for half in range(2):
                part_ref[:, half * width : (half + 1) * width] = partial(other, half)
                part_copy(block, half).start()
            for half in range(2):
                cols = slice(half * width, (half + 1) * width)
                mine = partial(side, half).astype(f32)
                part_copy(block, half).wait_recv()
                theirs = theirs_ref[block, :, cols].astype(f32)
                theirs_ref[block, :, cols] = (mine + theirs).astype(bf16)
            for half in range(2):
                part_copy(block, half).wait_send()

    def reply(step, way):
        block = here - step + 2 * way * step
        valid = (block >= 0) & (block < planes) & ((way == 0) | (step > 0))

        @pl.when(valid)
        def _():
            @pl.loop(0, group)
            def _(turn):
                i = lax.rem(place + turn, group)

                @pl.when(block * group + i != me)
                def _():
                    back(block, i).start()

                @pl.when(block * group + i == me)
                def _():
                    ret_ref[span(me * capacity, capacity)] = theirs_ref[
                        block, span(i * capacity, capacity)
                    ]

    def convolve():
        gated = c_ref[...].astype(f32) * u_ref[...].astype(f32)
        rim_gated = rim_ref[1].astype(f32) * rim_ref[0].astype(f32)
        row = lax.broadcasted_iota(jnp.int32, gated.shape, 0)
        one = jnp.where(row == 0, rim_gated[rim - 1 : rim], pltpu.roll(gated, 1, 0))
        two = jnp.where(
            row == 0,
            rim_gated[rim - 2 : rim - 1],
            jnp.where(row == 1, rim_gated[rim - 1 : rim], pltpu.roll(gated, 2, 0)),
        )
        conv = taps_ref[0:1, :] * two + taps_ref[1:2, :] * one + taps_ref[2:3, :] * gated
        return conv

    inside = (here > 0) & (here < planes - 1)

    @pl.loop(1, planes + 1)
    def _(step):
        with jax.named_scope("arrive0"):

            @pl.loop(0, 2)
            def _(piece):
                arrive(step, piece)

        with jax.named_scope("gather"):

            @pl.loop(0, 2)
            def _(way):
                gather(step - 1, way)

        @pl.loop(0, 2)
        def _(way):
            with jax.named_scope("compute"):
                compute(step - 1, way)

        with jax.named_scope("arrive2"):

            @pl.loop(2, 4)
            def _(piece):
                arrive(step, piece)

        @pl.loop(0, 2)
        def _(way):
            reply(step - 1, way)

        @pl.when(step == 1)
        def _():
            @pl.when(me > 0)
            def _():
                rims.wait_recv()

            mixed_value = b_ref[...].astype(f32) * convolve()
            near_ref[span(place * tokens, tokens)] = mixed_value.astype(bf16)

        @pl.when(step == jnp.where(inside, planes, 2))
        def _():
            @pl.loop(1, group)
            def _(i):
                mixed(i).start()

    loads[9].start()
    with jax.named_scope("wgrad"):

        for part in range(4):
            inputs = rows_ref[1, part]
            pieces[part][...] = contract_rows(inputs, gate_pre_ref[...])
            pieces[4 + part][...] = contract_rows(inputs, up_pre_ref[...])
            pieces[8 + part][...] = contract_rows(hidden_ref[...], rows_ref[0, part])

    @pl.loop(0, planes)
    def _(block):
        for way in range(2):
            room = here < planes - 1 if way == 0 else here > 0
            mine = block <= here if way == 0 else block >= here

            @pl.when(room & mine)
            def _():
                every(column.at[block], hop_send.at[way, block], hop_recv.at[0, 0]).wait_send()

    every(outgoing, cross_send, cross_recv.at[0, 0]).wait_send()
    spot = outgoing.at[:, :, pl.ds(0, (group - 1) * capacity)]
    every(spot, plane_send, plane_recv.at[0, 0]).wait_send()
    smalls.wait_send()

    @pl.when(me < count - 1)
    def _():
        rims.wait_send()

    swap(0).wait_send()

    @pl.loop(0, planes)
    def _(turn):
        block = lax.rem(here + turn, planes)
        with jax.named_scope("returned"):

            for_backs(block, lambda copy: copy.wait_recv())

        with jax.named_scope("pull"):
            rows = span(block * bunch, bunch)
            slot = lax.broadcasted_iota(jnp.int32, (tokens, bunch), 1) + block * bunch
            slot = slot.astype(f32)
            hit = (slot == spots_ref[:, 0:1]) | (slot == spots_ref[:, 1:2])
            pull = jnp.where(hit, 1.0, 0.0).astype(bf16)
            value = jnp.dot(pull, ret_ref[rows], preferred_element_type=f32)

            @pl.when(turn == 0)
            def _():
                total_ref[...] = value

            @pl.when(turn > 0)
            def _():
                total_ref[...] += value

    with jax.named_scope("cross"):
        total = jnp.zeros((tokens, lanes), f32)
        for start in range(0, 2 * width, lanes):
            cols = slice(start, start + lanes)
            total += grad_ref[:, cols].astype(f32) * gain_ref[:, cols] * total_ref[:, cols]
        inner_ref[...] = total
        swap(1).start()
        square = jnp.sum(square_ref[...] + square_other[...], axis=1, keepdims=True)
        inverse = lax.rsqrt(square / (4 * width) + EPSILON)
        swap(1).wait_recv()
        inner = jnp.sum(inner_ref[...] + inner_other[...], axis=1, keepdims=True)
        pull_back = inverse * inverse * inverse * inner / (4 * width)
        for piece in range(2):
            cols = slice(piece * width, (piece + 1) * width)
            grad_ref[:, cols] = (
                column[here, piece].astype(f32)
                + inverse * gain_ref[:, cols] * total_ref[:, cols]
                - grad_ref[:, cols].astype(f32) * pull_back
            ).astype(bf16)
        swap(2).start()

    upper = here >= planes // 2
    base = lax.div(here * parts, planes)

    def turned(k):
        return lax.rem(base + parts + jnp.where(upper, 1 + k, parts - 1 - k), parts)

    with jax.named_scope("spread"):

        if not plain:
            features = 2 * width
            run = near * sliver
            for start in range(0, features, sliver):
                goal = lax.broadcasted_iota(jnp.int32, (features, sliver), 1) + start
                inner_goal = lax.rem(goal, run)
                origin = (
                    lax.div(inner_goal, depth) * group + lax.div(goal, run)
                ) * depth + lax.rem(inner_goal, depth)
                match = lax.broadcasted_iota(jnp.int32, (features, sliver), 0) == origin
                turn_ref[:, start : start + sliver] = jnp.dot(
                    grad_ref[...],
                    jnp.where(match, 1.0, 0.0).astype(bf16),
                    preferred_element_type=f32,
                ).astype(bf16)

        def spread_all():
            @pl.loop(0, parts)
            def _(k):
                part = turned(k)

                @pl.when(owned(part))
                def _():
                    @pl.loop(0, group)
                    def _(target):
                        @pl.when(target != place)
                        def _():
                            spread(target, part).start()

                    block_ref[part, span(place * tokens, tokens)] = strip(place, part)[...]

        first = owned(turned(0))

        @pl.when(first)
        def _():
            spread_all()

    with jax.named_scope("mixer"):
        half = 2 * width
        loads[9].wait()
        mixer_grad = jnp.dot(
            grad_ref[...], gate_w[span(side * half, half)], preferred_element_type=f32
        )
        swap(2).wait_recv()
        mixer_grad += jnp.dot(
            grad_other[...], gate_w[span(other * half, half)], preferred_element_type=f32
        )
        delta = mixer_grad * b_ref[...].astype(f32)
        edge_ref[...] = delta[0 : edge_ref.shape[0]]

        @pl.when(me > 0)
        def _():
            edge_copy.start()

        b_out[...] = (mixer_grad * convolve()).astype(bf16)

    @pl.when(jnp.logical_not(first))
    def _():
        spread_all()

    mixes.wait()

    @pl.loop(0, parts)
    def _(k):
        part = turned(k)
        with jax.named_scope("collect"):

            @pl.when(owned(part))
            def _():
                spreads(part).wait_recv()
                hand(part).start()

            @pl.when(jnp.logical_not(owned(part)))
            def _():
                hand(part).wait_recv()

        with jax.named_scope("shares"):
            value = contract_rows(block_ref[part], near_ref[...])
            gate_pre_ref[span(part * sliver, sliver)] = value.astype(bf16)
            for j in range(per_part):

                @pl.when(part * per_part + j != here)
                def _():
                    share(part, j).start()

                @pl.when(part * per_part + j == here)
                def _():
                    proj_out[...] = value[j * depth : (j + 1) * depth]

    with jax.named_scope("edge"):

        @pl.when(me == count - 1)
        def _():
            edge_next[...] = jnp.zeros_like(edge_next)

        @pl.when(me < count - 1)
        def _():
            edge_copy.wait_recv()

        row = lax.broadcasted_iota(jnp.int32, delta.shape, 0)
        one = jnp.where(
            row == tokens - 1, edge_next[0:1], pltpu.roll(delta, tokens - 1, 0)
        )
        two = jnp.where(
            row == tokens - 2,
            edge_next[0:1],
            jnp.where(row == tokens - 1, edge_next[1:2], pltpu.roll(delta, tokens - 2, 0)),
        )
        gated_grad = taps_ref[2:3, :] * delta + taps_ref[1:2, :] * one + taps_ref[0:1, :] * two
        u_out[...] = (gated_grad * c_ref[...].astype(f32)).astype(bf16)
        c_out[...] = (gated_grad * u_ref[...].astype(f32)).astype(bf16)

    spot = ret_ref.at[pl.ds(0, (count - 1) * capacity)]
    every(spot, back_send, back_recv.at[0]).wait_send()

    @pl.when(me > 0)
    def _():
        edge_copy.wait_send()

    for i in range(1, 3):
        swap(i).wait_send()

    @pl.loop(0, parts)
    def _(part):
        @pl.when(owned(part))
        def _():
            spreads(part).wait_send()
            hand(part).wait_send()

    with jax.named_scope("final"):

        @pl.loop(1, planes)
        def _(i):
            source = lax.rem(here + i, planes)
            share_from(source).wait_recv()
            proj_out[...] += stack_ref[source].astype(f32)

    every(stack_ref.at[pl.ds(0, planes - 1)], share_send, share_recv.at[0]).wait_send()


def store_kernel(*refs):
    sources, targets, sems = refs[:17], refs[17:25], refs[25]
    copies = []
    for i in range(17):
        if i < 5:
            target = targets[i]
        else:
            which, part = (i - 5) // 4, (i - 5) % 4
            rows, cols = sources[i].shape
            target = targets[5 + which]
            if which < 2:
                target = target.at[pl.ds(part * rows, rows)]
            else:
                target = target.at[:, pl.ds(part * cols, cols)]
        copies.append(pltpu.make_async_copy(sources[i], target, sems.at[i]))
    for copy in copies:
        copy.start()
    for copy in copies:
        copy.wait()


def pinned(value):
    return pltpu.with_memory_space_constraint(value, pltpu.HBM)


def local(
    stream,
    norm_gain,
    cotangent,
    route_weights,
    routes,
    conv_input,
    conv_bgate,
    conv_cgate,
    conv_taps,
    out_proj,
    gate_weight,
    up_weight,
    down_weight,
):
    count = lax.axis_size("sp")
    group = 2 ** ((count.bit_length() - 1) // 2)
    planes = count // group
    tokens, features = stream.shape
    width = features // 2
    channels = conv_input.shape[1]
    gate_shape, down_shape = gate_weight.shape[1:], down_weight.shape[1:]
    hidden = gate_shape[1]
    capacity = 2 * tokens * routes.shape[1] // count
    bunch = group * capacity
    slots = count * capacity
    grant = 38 * MIB + 2 * planes * tokens * features * 2
    depth = 2 * features // count
    sliver = max(128, depth)
    parts = planes * depth // sliver
    f32, bf16 = jnp.float32, jnp.bfloat16
    shape = jax.ShapeDtypeStruct
    outs = (
        shape(stream.shape, bf16),
        shape((depth, channels), f32),
        shape(conv_input.shape, bf16),
        shape(conv_input.shape, bf16),
        shape(conv_input.shape, bf16),
        shape(gate_shape, f32),
        shape(gate_shape, f32),
        shape(down_shape, f32),
    )
    vmem, hbm = pl.BlockSpec(memory_space=pltpu.VMEM), pl.BlockSpec(memory_space=pltpu.HBM)
    dma = pltpu.SemaphoreType.DMA
    results = pl.pallas_call(
        lambda *refs: layer_kernel(planes, group, *refs),
        out_shape=tuple(pltpu.VMEM(out.shape, out.dtype) for out in outs[:5])
        + (pltpu.VMEM((width, hidden), f32),) * 8
        + (pltpu.VMEM((hidden, width), f32),) * 4,
        in_specs=[hbm] * 13,
        out_specs=[vmem] * 17,
        scratch_shapes=[
            pltpu.VMEM((1, features), f32),
            pltpu.VMEM(route_weights.shape[::-1], f32),
            pltpu.VMEM(routes.shape[::-1], jnp.int32),
            pltpu.VMEM(conv_taps.shape, f32),
            pltpu.VMEM((planes, 4, tokens, width), bf16),
            pltpu.VMEM((planes, 4, bunch, width), bf16),
            pltpu.VMEM((2, 4, slots, width), bf16),
            pltpu.VMEM(gate_shape, bf16),
            pltpu.VMEM(gate_shape, bf16),
            pltpu.VMEM(down_shape, bf16),
            pltpu.VMEM((slots, hidden), bf16),
            pltpu.VMEM((slots, hidden), bf16),
            pltpu.VMEM((slots, hidden), bf16),
            pltpu.VMEM((bunch, features), bf16),
            pltpu.VMEM((planes, bunch, features), bf16),
            pltpu.VMEM((slots, features), bf16),
            pltpu.VMEM((tokens, channels), bf16),
            pltpu.VMEM((tokens, channels), bf16),
            pltpu.VMEM((tokens, channels), bf16),
            pltpu.VMEM((group * tokens, channels), bf16),
            pltpu.VMEM((2, 16, channels), bf16),
            pltpu.VMEM((planes, 8, tokens), f32),
            pltpu.VMEM((tokens, 128), f32),
            pltpu.VMEM((tokens, 128), f32),
            pltpu.VMEM((tokens, 128), f32),
            pltpu.VMEM((tokens, 128), f32),
            pltpu.VMEM((2, bunch, tokens), bf16),
            pltpu.VMEM((tokens, 8), f32),
            pltpu.VMEM((tokens, features), f32),
            pltpu.VMEM((tokens, features), bf16),
            pltpu.VMEM((parts, group * tokens, sliver), bf16),
            pltpu.VMEM((planes, depth, channels), bf16),
            pltpu.VMEM((8, channels), f32),
            pltpu.VMEM((8, channels), f32),
            pltpu.VMEM(stream.shape if sliver > depth else (8, 128), bf16),
            dma((14,)),
            dma((2, planes)),
            dma((planes, 4)),
            dma,
            dma((planes, 4)),
            dma,
            dma((planes, 4)),
            dma((2,)),
            dma((planes, 2)),
            dma,
            dma((planes,)),
            dma,
            dma,
            dma,
            dma,
            dma((3,)),
            dma((3,)),
            dma,
            dma,
            dma((parts,)),
            dma((parts,)),
            dma((parts,)),
            dma((parts,)),
            dma,
            dma((planes,)),
            dma,
            dma,
        ],
        compiler_params=pltpu.CompilerParams(
            collective_id=0, has_side_effects=True, vmem_limit_bytes=grant
        ),
        name="layer",
    )(
        pinned(stream[None]),
        pinned(norm_gain[None, :]),
        pinned(cotangent[None]),
        pinned(route_weights.T),
        pinned(routes.T),
        pinned(conv_input[None]),
        pinned(conv_bgate[None]),
        pinned(conv_cgate[None]),
        pinned(conv_taps),
        pinned(out_proj[None]),
        pinned(gate_weight),
        pinned(up_weight),
        pinned(down_weight),
    )
    results = pl.pallas_call(
        store_kernel,
        out_shape=outs,
        in_specs=[vmem] * 17,
        out_specs=[hbm] * 8,
        scratch_shapes=[dma((17,))],
        compiler_params=pltpu.CompilerParams(vmem_limit_bytes=2**20),
        name="store",
    )(*results)
    return tuple(results[:5]) + tuple(value[None] for value in results[5:])


def solution(mesh):
    return jax.shard_map(
        local,
        mesh=mesh,
        in_specs=(
            P("sp", "tp"),
            P("tp"),
            P("sp", "tp"),
            P("sp", None),
            P("sp", None),
            P("sp", "tp"),
            P("sp", "tp"),
            P("sp", "tp"),
            P(None, "tp"),
            P(None, "tp"),
            P("sp", None, "tp"),
            P("sp", None, "tp"),
            P("sp", "tp", None),
        ),
        out_specs=(
            P("sp", "tp"),
            P("sp", "tp"),
            P("sp", "tp"),
            P("sp", "tp"),
            P("sp", "tp"),
            P("sp", None, "tp"),
            P("sp", None, "tp"),
            P("sp", "tp", None),
        ),
        check_vma=False,
    )
```
